256 devices in a mesh: sp: 32 (over z, x), tp: 8 (over y, core).
Axes of the slice: x: 4, y: 4, z: 8, core: 2. Of those that a mesh axis runs over, the one named last changes fastest.
Arguments:
- tokens: bfloat16 [12288, 2048], P('sp', 'tp'), may hold values from -6 to 6
- pre_gain: float32 [2048], replicated, may hold values from 0.1 to 1.9
- outer_gate_weight: bfloat16 [2048, 1024], P(None, 'tp'), may hold values from -0.125 to 0.125
- inner_gate_weight: bfloat16 [2048, 1024], P(None, 'tp'), may hold values from -0.125 to 0.125
- source_weight: bfloat16 [2048, 1024], P(None, 'tp'), may hold values from -0.125 to 0.125
- conv_taps: bfloat16 [3, 1024], P(None, 'tp'), may hold values from -3.5 to 3.5
- q_down_weight: bfloat16 [2048, 768], replicated, may hold values from -0.125 to 0.125
- q_norm_gain: float32 [768], replicated, may hold values from 0.5 to 16
- q_up_weight: bfloat16 [768, 3072], P(None, 'tp'), may hold values from -0.21875 to 0.21875
- kv_down_weight: bfloat16 [2048, 512], replicated, may hold values from -0.125 to 0.125
- rope_key_weight: bfloat16 [2048, 32], replicated, may hold values from -0.125 to 0.125
- kv_norm_gain: float32 [512], replicated, may hold values from 0.5 to 16
- kv_up_weight: bfloat16 [512, 4096], P(None, 'tp'), may hold values from -0.25 to 0.25
- attn_out_weight: bfloat16 [2048, 2048], P('tp'), may hold values from -4 to 4
- conv_out_weight: bfloat16 [1024, 2048], P('tp'), may hold values from -0.1875 to 0.1875
- post_gain: float32 [2048], P('tp'), may hold values from 0.1 to 1.9
Outputs:
- mixed: bfloat16 [12288, 2048], P('sp', 'tp')
- log_total: float32 [32, 12288], P('tp', 'sp')
The draws below stay inside these ranges and needn't reach their ends.
All inputs are finite; a program needn't handle non-finite values.
Results may differ from the reference program's by a relative error of at most 0.017.
The reference program's roundings to bfloat16 on the way count: a program that leaves them out, or rounds other values in their place, can miss the bound.
Values may be sent and summed in bfloat16 or wider, within the bound.
A program may use at most 128 MiB of HBM per device.

```python
import jax
import jax.numpy as jnp
from jax import lax

D = 2048
HEADS = 32
NOPE = 64
ROPE = 32
VDIM = 64
Q_RANK = 768
KV_RANK = 512
CONV_W = 1024
TAPS = 3
TOK_DEV = 384
TOKENS = 12288
N_SP = 32
N_TP = 8


def latent_gain(key, count):
    upper = 2.0
    return jnp.exp(jax.random.uniform(key, (count,), jnp.float32, jnp.log(0.5), jnp.log(upper)))


def draw_q_norm_gain(key, part):
    return latent_gain(jax.random.fold_in(key, 11), Q_RANK)


def draw_kv_norm_gain(key, part):
    return latent_gain(jax.random.fold_in(key, 23), KV_RANK)


def block_levels(stream_key, shape, shards, low, high):
    gain, own = 1.0, jax.random.fold_in(stream_key, 6)
    for dim, parts in shards:
        steps = jnp.exp(jax.random.uniform(jax.random.fold_in(own, dim), (parts,), jnp.float32, low / len(shards), high / len(shards)))
        gain = gain * jnp.repeat(steps, shape[dim] // parts).reshape([-1 if axis == dim else 1 for axis in range(len(shape))])
    return gain


def centred(stream_key, dims, scale, bound, split=(), held_as=jnp.bfloat16):
    values = scale * jax.random.normal(stream_key, dims, jnp.float32)
    if split:
        values = values * block_levels(stream_key, dims, split, -0.22, 0.18)
    return jnp.clip(values, -bound, bound).astype(held_as)


def setup_inputs(seed: int = 0) -> dict:
    splits = jax.random.split(jax.random.key(seed), 17)
    return {
        "tokens": centred(splits[0], (TOKENS, D), 1.0, 6.0, ((0, 32), (1, 8))),
        "pre_gain": jnp.clip(1.0 + 0.18 * jax.random.normal(splits[1], (D,), jnp.float32), 0.1, 1.9),
        "outer_gate_weight": centred(splits[2], (D, CONV_W), D ** -0.5, 0.125, ((1, 8),)),
        "inner_gate_weight": centred(splits[3], (D, CONV_W), D ** -0.5, 0.125, ((1, 8),)),
        "source_weight": centred(splits[4], (D, CONV_W), D ** -0.5, 0.125, ((1, 8),)),
        "conv_taps": centred(splits[5], (TAPS, CONV_W), TAPS ** -0.5, 3.5, ((1, 8),)),
        "q_down_weight": centred(splits[6], (D, Q_RANK), D ** -0.5, 0.125),
        "q_norm_gain": draw_q_norm_gain(jax.random.fold_in(splits[16], 71), 0),
        "q_up_weight": centred(splits[8], (Q_RANK, HEADS * (NOPE + ROPE)), Q_RANK ** -0.5, 0.21875, ((1, 8),)),
        "kv_down_weight": centred(splits[9], (D, KV_RANK), D ** -0.5, 0.125),
        "rope_key_weight": centred(splits[10], (D, ROPE), D ** -0.5, 0.125),
        "kv_norm_gain": draw_kv_norm_gain(jax.random.fold_in(splits[16], 71), 0),
        "kv_up_weight": centred(splits[12], (KV_RANK, HEADS * (NOPE + VDIM)), KV_RANK ** -0.5, 0.25, ((1, 8),)),
        "attn_out_weight": centred(splits[13], (HEADS * VDIM, D), 2 ** -0.5, 4.0, ((0, 8),)),
        "conv_out_weight": centred(splits[14], (CONV_W, D), CONV_W ** -0.5, 0.1875, ((0, 8),)),
        "post_gain": jnp.clip(1.0 + 0.18 * jax.random.normal(splits[15], (D,), jnp.float32), 0.1, 1.9),
    }


EPSILON = 1e-06
THETA = 500000.0

def rms_scale(values):
    return lax.rsqrt(lax.optimization_barrier(jnp.mean(values * values, axis=-1, keepdims=True)) + EPSILON)

def rotation(positions, width):
    freqs = THETA ** (-jnp.arange(0, width, 2, dtype=jnp.float32) / width)
    angles = positions.astype(jnp.float32)[:, None] * freqs[None, :]
    return (jnp.cos(angles), jnp.sin(angles))

def rotate(values, cosine, sine):
    half = values.shape[-1] // 2
    first = values[..., :half]
    second = values[..., half:]
    return jnp.concatenate([first * cosine - second * sine, second * cosine + first * sine], axis=-1)

def reference(tokens, pre_gain, outer_gate_weight, inner_gate_weight, source_weight, conv_taps, q_down_weight, q_norm_gain, q_up_weight, kv_down_weight, rope_key_weight, kv_norm_gain, kv_up_weight, attn_out_weight, conv_out_weight, post_gain):
    wide = tokens.astype(jnp.float32)
    scaled = (wide * pre_gain).astype(jnp.bfloat16)
    factor = rms_scale(wide)

    def project(weight):
        return jnp.dot(scaled, weight, preferred_element_type=jnp.float32) * factor
    outer = project(outer_gate_weight).astype(jnp.bfloat16)
    inner = project(inner_gate_weight).astype(jnp.bfloat16)
    source = project(source_weight).astype(jnp.bfloat16)
    driven = (inner.astype(jnp.float32) * source.astype(jnp.float32)).astype(jnp.bfloat16)
    padded = jnp.concatenate([jnp.zeros((TAPS - 1, CONV_W), jnp.bfloat16), driven], axis=0)
    convolved = jnp.zeros((TOKENS, CONV_W), jnp.float32)
    for index in range(TAPS):
        convolved = convolved + conv_taps[index].astype(jnp.float32) * padded[index:index + TOKENS].astype(jnp.float32)
    conv_branch = (outer.astype(jnp.float32) * convolved).astype(jnp.bfloat16)
    positions = jnp.arange(TOKENS, dtype=jnp.int32)
    cosine, sine = rotation(positions, ROPE)
    q_latent = project(q_down_weight)
    q_normed = (q_latent * rms_scale(q_latent) * q_norm_gain).astype(jnp.bfloat16)
    query = jnp.dot(q_normed, q_up_weight, preferred_element_type=jnp.float32).reshape(TOKENS, HEADS, NOPE + ROPE)
    q_plain = query[..., :NOPE].astype(jnp.bfloat16)
    q_turned = rotate(query[..., NOPE:], cosine[:, None], sine[:, None]).astype(jnp.bfloat16)
    kv_latent = project(kv_down_weight)
    latent = (kv_latent * rms_scale(kv_latent) * kv_norm_gain).astype(jnp.bfloat16)
    rope_key = rotate(project(rope_key_weight), cosine, sine).astype(jnp.bfloat16)
    keyvals = jnp.dot(latent, kv_up_weight, preferred_element_type=jnp.float32).astype(jnp.bfloat16)
    keyvals = keyvals.reshape(TOKENS, HEADS, NOPE + VDIM)
    head_plain = jnp.transpose(q_plain, (1, 0, 2))
    head_turned = jnp.transpose(q_turned, (1, 0, 2))
    head_keys = jnp.transpose(keyvals[..., :NOPE], (1, 0, 2))
    head_values = jnp.transpose(keyvals[..., NOPE:], (1, 0, 2))
    scale = (NOPE + ROPE) ** (-0.5)
    outputs = []
    logs = []
    for block in range(N_SP):
        first = block * TOK_DEV
        last = first + TOK_DEV
        key_turned = rope_key[:last]
        query_pos = jnp.arange(first, last, dtype=jnp.int32)
        key_pos = jnp.arange(last, dtype=jnp.int32)
        allowed = key_pos[None, :] <= query_pos[:, None]

        def per_head(items):
            plain, turned, keys, values = items
            scores = jnp.dot(plain, keys.T, preferred_element_type=jnp.float32)
            scores = scores + jnp.dot(turned, key_turned.T, preferred_element_type=jnp.float32)
            scores = jnp.where(allowed, scores * scale, -jnp.inf)
            maxima = lax.optimization_barrier(jnp.max(scores, axis=-1, keepdims=True))
            weights = jnp.exp(scores - maxima)
            totals = lax.optimization_barrier(jnp.sum(weights, axis=-1))
            result = jnp.dot(weights.astype(jnp.bfloat16), values, preferred_element_type=jnp.float32) / totals[:, None]
            return (result.astype(jnp.bfloat16), maxima[:, 0] + jnp.log(totals))
        block_out, block_log = lax.map(per_head, (head_plain[:, first:last], head_turned[:, first:last], head_keys[:, :last], head_values[:, :last]))
        outputs.append(block_out)
        logs.append(block_log)
    attended = jnp.concatenate(outputs, axis=1)
    log_total = jnp.concatenate(logs, axis=1)
    attended = jnp.transpose(attended, (1, 0, 2)).reshape(TOKENS, HEADS * VDIM)
    head_rows = HEADS // N_TP * VDIM
    channel_rows = CONV_W // N_TP
    projected = jnp.zeros((TOKENS, D), jnp.float32)
    for group in range(N_TP):
        head_part = jnp.dot(attended[:, group * head_rows:(group + 1) * head_rows], attn_out_weight[group * head_rows:(group + 1) * head_rows], preferred_element_type=jnp.float32)
        conv_part = jnp.dot(conv_branch[:, group * channel_rows:(group + 1) * channel_rows], conv_out_weight[group * channel_rows:(group + 1) * channel_rows], preferred_element_type=jnp.float32)
        rounded = lax.optimization_barrier((head_part + conv_part).astype(jnp.bfloat16))
        projected = projected + rounded.astype(jnp.float32)
    mixed = (projected * rms_scale(projected) * post_gain).astype(jnp.bfloat16)
    return (mixed, log_total)
```

```python
import functools
import math

import jax
import jax.numpy as jnp
from jax import lax
from jax.experimental import pallas as pl
from jax.experimental.pallas import tpu as pltpu
from jax.sharding import PartitionSpec as P

D = 2048
NOPE = 64
ROPE = 32
VDIM = 64
TAPS = 3
NZ, NX, NY = 8, 4, 4
ROWS = 384
KVR = NOPE + ROPE + VDIM
QK = NOPE + ROPE
LOCAL = 4
BLOCKS = NZ * NX

EPSILON = 1e-06
THETA = 500000.0
NEGATIVE = -1e30
LOG2E = math.log2(math.e)
MESH = pl.DeviceIdType.MESH
VMEM = pltpu.MemorySpace.VMEM


def side(z):
    return lax.rem(lax.div(z + 1, 2), 2)


def plane(j, core):
    return 2 * j + lax.rem(j + core, 2)


def remote(src, dst, send, recv, sp, tp):
    return pltpu.make_async_remote_copy(
        src_ref=src, dst_ref=dst, send_sem=send, recv_sem=recv,
        device_id=(sp, tp), device_id_type=MESH,
    )


def greet(peers):
    barrier = pltpu.get_barrier_semaphore()
    for sp, tp in peers:
        pl.semaphore_signal(barrier, inc=1, device_id=(sp, tp), device_id_type=MESH)
    pl.semaphore_wait(barrier, len(peers))


def gather_kernel(part_ref, out_ref, y_send, y_recv, d_send, d_recv):
    sp = lax.axis_index("sp")
    tp = lax.axis_index("tp")
    core = lax.rem(tp, 2)
    y = lax.div(tp, 2)
    mate = tp + 1 - 2 * core
    up = lax.rem(y + 1, NY) * 2 + core
    down = lax.rem(y + NY - 1, NY) * 2 + core
    far = lax.rem(y + 2, NY) * 2 + core
    rows, width = part_ref.shape
    half = rows // 2

    def slot(owner, first=0, count=rows):
        return out_ref.at[pl.ds(first, count), pl.ds(pl.multiple_of(owner * width, width), width)]

    greet([(sp, mate), (sp, up), (sp, down)])
    copies = []

    def send(src, dst, s, r, to):
        c = remote(src, dst, s, r, sp, to)
        c.start()
        copies.append(c)

    send(part_ref, slot(tp), y_send.at[0], y_recv.at[0], up)
    send(part_ref, slot(tp), y_send.at[1], y_recv.at[1], down)
    send(part_ref, slot(tp), d_send.at[0], d_recv.at[0], mate)
    out_ref[:, pl.ds(pl.multiple_of(tp * width, width), width)] = part_ref[...]

    def arrived(index, owner, first=0, count=rows):
        remote(slot(owner, first, count), slot(owner, first, count),
               y_send.at[index], y_recv.at[index], sp, up).wait_recv()

    arrived(0, down)
    send(slot(down, 0, half), slot(down, 0, half), y_send.at[2], y_recv.at[2], up)
    send(slot(down), slot(down), d_send.at[1], d_recv.at[1], mate)
    arrived(1, up)
    send(slot(up, half, half), slot(up, half, half), y_send.at[3], y_recv.at[3], down)
    send(slot(up), slot(up), d_send.at[2], d_recv.at[2], mate)
    arrived(2, far, 0, half)
    send(slot(far, 0, half), slot(far, 0, half), d_send.at[3], d_recv.at[3], mate)
    arrived(3, far, half, half)
    send(slot(far, half, half), slot(far, half, half), d_send.at[4], d_recv.at[4], mate)

    other = 1 - 2 * core
    for index, (owner, first, count) in enumerate(
        [(mate, 0, rows), (down + other, 0, rows), (up + other, 0, rows),
         (far + other, 0, half), (far + other, half, half)]
    ):
        remote(slot(owner, first, count), slot(owner, first, count),
               d_send.at[index], d_recv.at[index], sp, mate).wait_recv()
    for c in copies:
        c.wait_send()


def gathered(part, collective_id):
    rows, width = part.shape
    return pl.pallas_call(
        gather_kernel,
        out_shape=jax.ShapeDtypeStruct((rows, width * 2 * NY), part.dtype),
        in_specs=[pl.BlockSpec(memory_space=VMEM)],
        out_specs=pl.BlockSpec(memory_space=VMEM),
        scratch_shapes=[
            pltpu.SemaphoreType.DMA((4,)),
            pltpu.SemaphoreType.DMA((4,)),
            pltpu.SemaphoreType.DMA((5,)),
            pltpu.SemaphoreType.DMA((5,)),
        ],
        compiler_params=pltpu.CompilerParams(collective_id=collective_id, has_side_effects=True),
        name="gather_tp",
    )(part)


def exchange_kernel(kv_ref, q_ref, all_ref, mine_ref,
                    kz_send, kz_recv, qz_send, qz_recv, x_send, x_recv, d_send, d_recv):
    sp = lax.axis_index("sp")
    tp = lax.axis_index("tp")
    z, x = lax.div(sp, NX), lax.rem(sp, NX)
    core, y = lax.rem(tp, 2), lax.div(tp, 2)
    mate = tp + 1 - 2 * core
    xp, xm, xf = (lax.rem(x + k, NX) for k in (1, NX - 1, 2))
    to_core = side(z)
    owner = lax.div(z, LOCAL)
    half = KVR // 2

    peers = [(lax.rem(z + k, NZ) * NX + x, 2 * y + c) for k in range(1, NZ) for c in (0, 1)]
    peers += [(sp, mate), (z * NX + xp, tp), (z * NX + xm, tp)]
    greet(peers)

    keep = jnp.logical_and(owner == core, to_core == core)
    own_head = z - LOCAL * core

    def z_copies(h):
        target = LOCAL * core + h
        return (
            remote(kv_ref.at[h], all_ref.at[sp], kz_send.at[h], kz_recv.at[lax.div(z, 2)],
                   target * NX + x, 2 * y + to_core),
            remote(q_ref.at[h], mine_ref.at[lax.div(z, 2)], qz_send.at[h],
                   qz_recv.at[lax.div(z, 2)], target * NX + x, 2 * y + to_core),
        )

    def leaves(h):
        return jnp.logical_not(jnp.logical_and(keep, own_head == h))

    for which in (0, 1):
        for h in range(LOCAL):
            @pl.when(leaves(h))
            def _(h=h):
                z_copies(h)[which].start()

    for h in range(LOCAL):
        @pl.when(jnp.logical_not(leaves(h)))
        def _(h=h):
            all_ref[sp] = kv_ref[h]
            mine_ref[lax.div(z, 2)] = q_ref[h]

    first = lax.div(z, 2)
    order = [lax.rem(first + k, 4) for k in (0, 1, 3, 2)]
    sends = []

    def send(src, s, r, to_sp, to_tp):
        c = remote(src, src, s, r, to_sp, to_tp)
        c.start()
        sends.append(c)

    def z_wait(j, dst, send_sem, recv_sem):
        from_plane = plane(j, core)

        @pl.when(jnp.logical_not(jnp.logical_and(keep, from_plane == z)))
        def _():
            remote(dst, dst, send_sem, recv_sem, sp, mate).wait_recv()

    def z_stage(j):
        block = all_ref.at[plane(j, core) * NX + x]
        z_wait(j, block, kz_send.at[0], kz_recv.at[j])
        send(block, x_send.at[j, 0], x_recv.at[j, 0], z * NX + xp, tp)
        send(block, x_send.at[j, 1], x_recv.at[j, 1], z * NX + xm, tp)
        send(block, d_send.at[j, 0], d_recv.at[j, 0], sp, mate)

    def wait(dst, sems, index):
        remote(dst, dst, sems[0].at[index], sems[1].at[index], sp, mate).wait_recv()

    def x_stage(j):
        base = plane(j, core) * NX
        wait(all_ref.at[base + xm], (x_send, x_recv), (j, 0))
        send(all_ref.at[base + xm, pl.ds(0, half)], x_send.at[j, 2], x_recv.at[j, 2], z * NX + xp, tp)
        send(all_ref.at[base + xm], d_send.at[j, 1], d_recv.at[j, 1], sp, mate)
        wait(all_ref.at[base + xp], (x_send, x_recv), (j, 1))
        send(all_ref.at[base + xp, pl.ds(half, half)], x_send.at[j, 3], x_recv.at[j, 3], z * NX + xm, tp)
        send(all_ref.at[base + xp], d_send.at[j, 2], d_recv.at[j, 2], sp, mate)

    def far_stage(j):
        base = plane(j, core) * NX
        for k in (0, 1):
            part = all_ref.at[base + xf, pl.ds(k * half, half)]
            wait(part, (x_send, x_recv), (j, 2 + k))
            send(part, d_send.at[j, 3 + k], d_recv.at[j, 3 + k], sp, mate)

    for step in range(6):
        if step < 4:
            z_stage(order[step])
        if 1 <= step < 5:
            x_stage(order[step - 1])
        if step >= 2:
            far_stage(order[step - 2])

    for j in range(4):
        base = plane(j, 1 - core) * NX
        wait(all_ref.at[base + x], (d_send, d_recv), (j, 0))
        wait(all_ref.at[base + xm], (d_send, d_recv), (j, 1))
        wait(all_ref.at[base + xp], (d_send, d_recv), (j, 2))
        for k in (0, 1):
            wait(all_ref.at[base + xf, pl.ds(k * half, half)], (d_send, d_recv), (j, 3 + k))
        z_wait(j, mine_ref.at[j], qz_send.at[0], qz_recv.at[j])
    for c in sends:
        c.wait_send()
    for h in range(LOCAL):
        @pl.when(leaves(h))
        def _(h=h):
            for c in z_copies(h):
                c.wait_send()


def exchanged(kv, q):
    return pl.pallas_call(
        exchange_kernel,
        out_shape=(
            jax.ShapeDtypeStruct((BLOCKS, KVR, ROWS), kv.dtype),
            jax.ShapeDtypeStruct((LOCAL, QK, ROWS), q.dtype),
        ),
        in_specs=[pl.BlockSpec(memory_space=VMEM)] * 2,
        out_specs=(pl.BlockSpec(memory_space=VMEM),) * 2,
        scratch_shapes=[
            pltpu.SemaphoreType.DMA((4,)),
            pltpu.SemaphoreType.DMA((4,)),
            pltpu.SemaphoreType.DMA((4,)),
            pltpu.SemaphoreType.DMA((4,)),
            pltpu.SemaphoreType.DMA((4, 4)),
            pltpu.SemaphoreType.DMA((4, 4)),
            pltpu.SemaphoreType.DMA((4, 5)),
            pltpu.SemaphoreType.DMA((4, 5)),
        ],
        compiler_params=pltpu.CompilerParams(collective_id=1, has_side_effects=True),
        name="heads_to_planes",
    )(kv, q)


def attention_kernel(kv_ref, q_ref, out_ref, log_ref, keys, m_ref, l_ref, acc_ref):
    sp = lax.axis_index("sp")
    core = lax.rem(lax.axis_index("tp"), 2)
    x = lax.rem(sp, NX)
    factor = QK ** -0.5 * LOG2E

    def turn(kb, carry):
        keys[kb] = kv_ref[kb, 0:QK, :].astype(jnp.float32).T.astype(jnp.bfloat16)
        return carry

    lax.fori_loop(0, BLOCKS, turn, 0)

    for j in range(LOCAL):
        own = plane(j, core) * NX + x
        m_ref[...] = jnp.full_like(m_ref, NEGATIVE)
        l_ref[...] = jnp.zeros_like(l_ref)
        acc_ref[...] = jnp.zeros_like(acc_ref)
        query = q_ref[j]

        def step(kb, masked):
            scores = jnp.dot(keys[kb], query, preferred_element_type=jnp.float32) * factor
            if masked:
                key = lax.broadcasted_iota(jnp.int32, scores.shape, 0)
                row = lax.broadcasted_iota(jnp.int32, scores.shape, 1)
                scores = jnp.where(key <= row, scores, NEGATIVE)
            old = m_ref[...]
            fresh = jnp.maximum(old, jnp.max(scores, axis=0, keepdims=True))
            shrink = jnp.exp2(old - fresh)
            weights = jnp.exp2(scores - fresh)
            m_ref[...] = fresh
            l_ref[...] = l_ref[...] * shrink + jnp.sum(weights, axis=0, keepdims=True)
            acc_ref[...] = acc_ref[...] * shrink + jnp.dot(
                kv_ref[kb, QK:KVR, :], weights.astype(jnp.bfloat16),
                preferred_element_type=jnp.float32,
            )

        def advance(kb, carry):
            step(kb, False)
            return carry

        lax.fori_loop(0, own, advance, 0)
        step(own, True)
        out_ref[j] = (acc_ref[...] / l_ref[...]).astype(jnp.bfloat16)
        total = m_ref[...] * (1.0 / LOG2E) + jnp.log(l_ref[...])
        log_ref[j] = jnp.broadcast_to(total, (8, ROWS))


def attended_heads(kv, q):
    return pl.pallas_call(
        attention_kernel,
        out_shape=(
            jax.ShapeDtypeStruct((LOCAL, VDIM, ROWS), jnp.bfloat16),
            jax.ShapeDtypeStruct((LOCAL, 8, ROWS), jnp.float32),
        ),
        in_specs=[pl.BlockSpec(memory_space=VMEM)] * 2,
        out_specs=(pl.BlockSpec(memory_space=VMEM),) * 2,
        scratch_shapes=[
            pltpu.VMEM((BLOCKS, ROWS, QK), jnp.bfloat16),
            pltpu.VMEM((1, ROWS), jnp.float32),
            pltpu.VMEM((1, ROWS), jnp.float32),
            pltpu.VMEM((VDIM, ROWS), jnp.float32),
        ],
        cost_estimate=pl.CostEstimate(flops=6 * 10**9, bytes_accessed=10**7, transcendentals=10**7),
        name="attention",
    )(kv, q)


def return_kernel(out_ref, log_ref, all_ref, logs_ref, a_send, a_recv, b_send, b_recv):
    sp = lax.axis_index("sp")
    tp = lax.axis_index("tp")
    z, x = lax.div(sp, NX), lax.rem(sp, NX)
    core, y = lax.rem(tp, 2), lax.div(tp, 2)
    mate = tp + 1 - 2 * core
    greet([(lax.rem(z + k, NZ) * NX + x, 2 * y + c) for k in range(1, NZ) for c in (0, 1)]
          + [(sp, mate)])
    to = 2 * y + lax.div(z, LOCAL)
    head = lax.rem(z, LOCAL)

    def copies(j):
        target = plane(j, core) * NX + x
        return (
            remote(out_ref.at[j], all_ref.at[head], a_send.at[j], a_recv.at[head], target, to),
            remote(log_ref.at[j], logs_ref.at[head], b_send.at[j], b_recv.at[head], target, to),
        )

    keep = jnp.logical_and(to == tp, side(z) == core)

    def leaves(j):
        return jnp.logical_not(jnp.logical_and(keep, plane(j, core) == z))

    for which in (0, 1):
        for j in range(LOCAL):
            @pl.when(leaves(j))
            def _(j=j):
                copies(j)[which].start()
    for j in range(LOCAL):
        @pl.when(jnp.logical_not(leaves(j)))
        def _(j=j):
            all_ref[head] = out_ref[j]
            logs_ref[head] = log_ref[j]
    for h in range(LOCAL):
        @pl.when(jnp.logical_not(jnp.logical_and(keep, LOCAL * core + h == z)))
        def _(h=h):
            remote(all_ref.at[h], all_ref.at[h], a_send.at[h], a_recv.at[h], sp, mate).wait_recv()
            remote(logs_ref.at[h], logs_ref.at[h], b_send.at[h], b_recv.at[h], sp, mate).wait_recv()
    for j in range(LOCAL):
        @pl.when(leaves(j))
        def _(j=j):
            for c in copies(j):
                c.wait_send()


def returned(out, log):
    return pl.pallas_call(
        return_kernel,
        out_shape=(
            jax.ShapeDtypeStruct(out.shape, out.dtype),
            jax.ShapeDtypeStruct(log.shape, log.dtype),
        ),
        in_specs=[pl.BlockSpec(memory_space=VMEM)] * 2,
        out_specs=(pl.BlockSpec(memory_space=VMEM),) * 2,
        scratch_shapes=[pltpu.SemaphoreType.DMA((4,))] * 4,
        compiler_params=pltpu.CompilerParams(collective_id=2, has_side_effects=True),
        name="results_to_rows",
    )(out, log)


def copy_for_each(shard, axis):
    peers = lax.axis_size(axis)
    return lax.all_to_all(
        jnp.broadcast_to(shard[None], (peers, *shard.shape)), axis, 0, 0, tiled=True
    )


def from_behind(value, axis, steps):
    count = lax.axis_size(axis)
    leading, last = (max(0, -steps), min(count, count - steps))
    return lax.ppermute(value, axis, [(source, source + steps) for source in range(leading, last)])


def cut_along(shard, dim, peers):
    lengths = shard.shape
    pieces = shard.reshape(*lengths[:dim], peers, lengths[dim] // peers, *lengths[dim + 1 :])
    return jnp.moveaxis(pieces, dim, 0)


def summed_on_arrival(shard, axis, dim):
    peers = lax.axis_size(axis)
    pieces = lax.all_to_all(cut_along(shard, dim, peers), axis, 0, 0, tiled=True)
    return jnp.sum(pieces.astype(jnp.float32), axis=0)


def over_copies(shard, axis):
    return copy_for_each(shard, axis).sum(axis=0)


def rms_factor(values):
    return lax.rsqrt(jnp.mean(values * values, axis=-1, keepdims=True) + EPSILON)


def rotation(positions, width):
    freqs = THETA ** (-jnp.arange(0, width, 2, dtype=jnp.float32) / width)
    angles = freqs[:, None] * positions.astype(jnp.float32)[None, :]
    return (jnp.cos(angles), jnp.sin(angles))


def rotate(values, cosine, sine):
    half = values.shape[-2] // 2
    first = values[..., :half, :]
    second = values[..., half:, :]
    return jnp.concatenate(
        [first * cosine - second * sine, second * cosine + first * sine], axis=-2
    )


def dot_turned(weight, rows):
    return lax.dot_general(
        weight, rows, (((0,), (1,)), ((), ())), preferred_element_type=jnp.float32
    )


def body(
    tokens,
    pre_gain,
    outer_gate_weight,
    inner_gate_weight,
    source_weight,
    conv_taps,
    q_down_weight,
    q_norm_gain,
    q_up_weight,
    kv_down_weight,
    rope_key_weight,
    kv_norm_gain,
    kv_up_weight,
    attn_out_weight,
    conv_out_weight,
    post_gain,
):
    token_rows = tokens.shape[0]
    wide = gathered(tokens, 0).astype(jnp.float32)
    scaled = (wide * pre_gain).astype(jnp.bfloat16)
    squares = jnp.sum(wide * wide, axis=1)
    factor = lax.rsqrt(squares / D + EPSILON)[:, None]

    def project(weight):
        return jnp.dot(scaled, weight, preferred_element_type=jnp.float32) * factor

    query_pos = lax.axis_index("sp") * token_rows + jnp.arange(token_rows, dtype=jnp.int32)
    cosine, sine = rotation(query_pos, ROPE)
    q_latent = project(q_down_weight)
    q_normed = (q_latent * rms_factor(q_latent) * q_norm_gain).astype(jnp.bfloat16)
    query = dot_turned(q_up_weight, q_normed).reshape(LOCAL, QK, token_rows)
    q_send = jnp.concatenate(
        [query[:, :NOPE], rotate(query[:, NOPE:], cosine, sine)], axis=1
    ).astype(jnp.bfloat16)
    kv_latent = project(kv_down_weight)
    latent = (kv_latent * rms_factor(kv_latent) * kv_norm_gain).astype(jnp.bfloat16)
    rope_key = rotate(project(rope_key_weight).T, cosine, sine).astype(jnp.bfloat16)
    keyvals = dot_turned(kv_up_weight, latent).astype(jnp.bfloat16)
    keyvals = keyvals.reshape(LOCAL, NOPE + VDIM, token_rows)
    kv_send = jnp.concatenate(
        [
            keyvals[:, :NOPE],
            jnp.broadcast_to(rope_key[None], (LOCAL, ROPE, token_rows)),
            keyvals[:, NOPE:],
        ],
        axis=1,
    )

    outer = project(outer_gate_weight).astype(jnp.bfloat16)
    inner = project(inner_gate_weight).astype(jnp.bfloat16)
    source = project(source_weight).astype(jnp.bfloat16)
    driven = (inner.astype(jnp.float32) * source.astype(jnp.float32)).astype(jnp.bfloat16)
    prior = from_behind(driven[token_rows - (TAPS - 1) :], "sp", 1)
    extended = jnp.concatenate([prior, driven], axis=0)
    convolved = jnp.zeros(driven.shape, jnp.float32)
    for index in range(TAPS):
        convolved = convolved + conv_taps[index].astype(jnp.float32) * extended[
            index : index + token_rows
        ].astype(jnp.float32)
    conv_branch = (outer.astype(jnp.float32) * convolved).astype(jnp.bfloat16)

    kv_all, q_mine = exchanged(kv_send, q_send)
    out, log = attended_heads(kv_all, q_mine)
    heads, logs = returned(out, log)
    log_total = logs[:, 0, :]
    attended = heads.reshape(LOCAL * VDIM, token_rows)
    partial_value = lax.dot_general(
        attended, attn_out_weight, (((0,), (0,)), ((), ())), preferred_element_type=jnp.float32
    )
    partial_value = partial_value + jnp.dot(
        conv_branch, conv_out_weight, preferred_element_type=jnp.float32
    )
    summed = summed_on_arrival(partial_value.astype(jnp.bfloat16), "tp", 1)
    row_squares = over_copies(jnp.sum(summed * summed, axis=1), "tp")
    mixed = summed * lax.rsqrt(row_squares / D + EPSILON)[:, None] * post_gain
    return (mixed.astype(jnp.bfloat16), log_total)


def solution(mesh):
    placed = (
        P("sp", "tp"),
        P(),
        P(None, "tp"),
        P(None, "tp"),
        P(None, "tp"),
        P(None, "tp"),
        P(),
        P(),
        P(None, "tp"),
        P(),
        P(),
        P(),
        P(None, "tp"),
        P("tp", None),
        P("tp", None),
        P("tp"),
    )
    return jax.shard_map(
        body, mesh=mesh, in_specs=placed, out_specs=(P("sp", "tp"), P("tp", "sp")), check_vma=False
    )
```

```python
import functools
import math

import jax
import jax.numpy as jnp
from jax import lax
from jax.experimental import pallas as pl
from jax.experimental.pallas import tpu as pltpu
from jax.sharding import PartitionSpec as P

D = 2048
NOPE = 64
ROPE = 32
VDIM = 64
TAPS = 3
NZ, NX, NY = 8, 4, 4
ROWS = 384
KVR = NOPE + ROPE + VDIM
QK = NOPE + ROPE
LOCAL = 4
BLOCKS = NZ * NX

EPSILON = 1e-06
THETA = 500000.0
NEGATIVE = -1e30
LOG2E = math.log2(math.e)
MESH = pl.DeviceIdType.MESH
VMEM = pltpu.MemorySpace.VMEM


def side(z):
    return lax.rem(lax.div(z + 1, 2), 2)


def plane(j, core):
    return 2 * j + lax.rem(j + core, 2)


def remote(src, dst, send, recv, sp, tp):
    return pltpu.make_async_remote_copy(
        src_ref=src, dst_ref=dst, send_sem=send, recv_sem=recv,
        device_id=(sp, tp), device_id_type=MESH,
    )


def greet(peers):
    barrier = pltpu.get_barrier_semaphore()
    for sp, tp in peers:
        pl.semaphore_signal(barrier, inc=1, device_id=(sp, tp), device_id_type=MESH)
    pl.semaphore_wait(barrier, len(peers))


def gather_kernel(part_ref, out_ref, y_send, y_recv, d_send, d_recv):
    sp = lax.axis_index("sp")
    tp = lax.axis_index("tp")
    core = lax.rem(tp, 2)
    y = lax.div(tp, 2)
    mate = tp + 1 - 2 * core
    up = lax.rem(y + 1, NY) * 2 + core
    down = lax.rem(y + NY - 1, NY) * 2 + core
    far = lax.rem(y + 2, NY) * 2 + core
    rows, width = part_ref.shape
    half = rows // 2

    def slot(owner, first=0, count=rows):
        return out_ref.at[pl.ds(first, count), pl.ds(pl.multiple_of(owner * width, width), width)]

    greet([(sp, mate), (sp, up), (sp, down)])
    copies = []

    def send(src, dst, s, r, to):
        c = remote(src, dst, s, r, sp, to)
        c.start()
        copies.append(c)

    send(part_ref, slot(tp), y_send.at[0], y_recv.at[0], up)
    send(part_ref, slot(tp), y_send.at[1], y_recv.at[1], down)
    send(part_ref, slot(tp), d_send.at[0], d_recv.at[0], mate)
    out_ref[:, pl.ds(pl.multiple_of(tp * width, width), width)] = part_ref[...]

    def arrived(index, owner, first=0, count=rows):
        remote(slot(owner, first, count), slot(owner, first, count),
               y_send.at[index], y_recv.at[index], sp, up).wait_recv()

    arrived(0, down)
    send(slot(down, 0, half), slot(down, 0, half), y_send.at[2], y_recv.at[2], up)
    send(slot(down), slot(down), d_send.at[1], d_recv.at[1], mate)
    arrived(1, up)
    send(slot(up, half, half), slot(up, half, half), y_send.at[3], y_recv.at[3], down)
    send(slot(up), slot(up), d_send.at[2], d_recv.at[2], mate)
    arrived(2, far, 0, half)
    send(slot(far, 0, half), slot(far, 0, half), d_send.at[3], d_recv.at[3], mate)
    arrived(3, far, half, half)
    send(slot(far, half, half), slot(far, half, half), d_send.at[4], d_recv.at[4], mate)

    other = 1 - 2 * core
    for index, (owner, first, count) in enumerate(
        [(mate, 0, rows), (down + other, 0, rows), (up + other, 0, rows),
         (far + other, 0, half), (far + other, half, half)]
    ):
        remote(slot(owner, first, count), slot(owner, first, count),
               d_send.at[index], d_recv.at[index], sp, mate).wait_recv()
    for c in copies:
        c.wait_send()


def gathered(part, collective_id):
    rows, width = part.shape
    return pl.pallas_call(
        gather_kernel,
        out_shape=jax.ShapeDtypeStruct((rows, width * 2 * NY), part.dtype),
        in_specs=[pl.BlockSpec(memory_space=VMEM)],
        out_specs=pl.BlockSpec(memory_space=VMEM),
        scratch_shapes=[
            pltpu.SemaphoreType.DMA((4,)),
            pltpu.SemaphoreType.DMA((4,)),
            pltpu.SemaphoreType.DMA((5,)),
            pltpu.SemaphoreType.DMA((5,)),
        ],
        compiler_params=pltpu.CompilerParams(collective_id=collective_id, has_side_effects=True),
        name="gather_tp",
    )(part)


def attention_step(kv_ref, q_ref, m_ref, l_ref, acc_ref, block, group, active, offset):
    scale = QK ** -0.5 * LOG2E
    width = active * ROWS
    cols = slice(0, width)
    scores = []
    for g in range(group):
        keys = kv_ref[block + g, 0:QK, :].T
        value = jnp.dot(keys, q_ref[:, cols], preferred_element_type=jnp.float32)
        if offset is not None:
            start = width - ROWS
            key = lax.broadcasted_iota(jnp.int32, value.shape, 0) + (offset + g * ROWS)
            row = lax.broadcasted_iota(jnp.int32, value.shape, 1) - start
            keep = key <= row
            if start:
                keep = jnp.logical_or(keep, row < 0)
            value = jnp.where(keep, value, NEGATIVE)
        scores.append(value)
    old = m_ref[:, cols]
    top = functools.reduce(jnp.maximum, [jnp.max(v, axis=0, keepdims=True) for v in scores])
    fresh = jnp.maximum(old, top * scale)
    shrink = jnp.exp2(old - fresh)
    weights = [jnp.exp2(v * scale - fresh) for v in scores]
    m_ref[:, cols] = fresh
    l_ref[:, cols] = l_ref[:, cols] * shrink + sum(
        jnp.sum(w, axis=0, keepdims=True) for w in weights
    )
    acc_ref[:, cols] = acc_ref[:, cols] * shrink + sum(
        jnp.dot(kv_ref[block + g, QK:KVR, :], w.astype(jnp.bfloat16), preferred_element_type=jnp.float32)
        for g, w in enumerate(weights)
    )


GROUPS = {4: 1, 3: 1, 2: 2, 1: 4}


def attend_plane(kv_ref, q_ref, state, p, core, x):
    direct = side(p) == core
    pair = lax.div(p, 2)
    later = LOCAL - pair - lax.rem(p, 2)
    for active in range(1, LOCAL + 1):
        group = GROUPS[active]

        @pl.when(jnp.logical_and(direct, pair == LOCAL - active))
        def _(active=active, group=group):
            def advance(i, carry):
                attention_step(kv_ref, q_ref, *state, p * NX + i * group, group, active,
                               (i * group - x) * ROWS)
                return carry

            lax.fori_loop(0, NX // group, advance, 0)

        @pl.when(jnp.logical_and(jnp.logical_not(direct), later == active))
        def _(active=active, group=group):
            def advance(i, carry):
                attention_step(kv_ref, q_ref, *state, p * NX + i * group, group, active, None)
                return carry

            lax.fori_loop(0, NX // group, advance, 0)


def layer_kernel(
    kv_ref, q_ref, conv_ref, gain_ref, wa_ref, wc_ref,
    mixed_ref, logs_ref,
    all_ref, mine_ref, wcol, wconv, convs, heads, results, logs, stats, m_ref, l_ref, acc_ref,
    kz_send, kz_recv, qz_send, qz_recv, x_send, x_recv, d_send, d_recv,
    wa_send, wa_recv, wc_send, wc_recv, cy_send, cy_recv, cd_send, cd_recv,
    rz_send, rz_recv, lz_send, lz_recv, hy_send, hy_recv, hd_send, hd_recv, s_send, s_recv,
):
    sp = lax.axis_index("sp")
    tp = lax.axis_index("tp")
    z, x = lax.div(sp, NX), lax.rem(sp, NX)
    core, y = lax.rem(tp, 2), lax.div(tp, 2)
    other = 1 - core
    mate = tp + 1 - 2 * core
    xp, xm, xf = (lax.rem(x + k, NX) for k in (1, NX - 1, 2))
    up, down, far = (lax.rem(y + k, NY) * 2 + core for k in (1, NY - 1, 2))
    flip = other - core
    to_core = side(z)
    owner = lax.div(z, LOCAL)
    half = KVR // 2
    n_tp = 2 * NY

    peers = [(lax.rem(z + k, NZ) * NX + x, 2 * y + c) for k in range(1, NZ) for c in (0, 1)]
    peers += [(z * NX + xp, tp), (z * NX + xm, tp)]
    peers += [(sp, lax.rem(tp + k, n_tp)) for k in range(1, n_tp)]
    greet(peers)

    keep = jnp.logical_and(owner == core, to_core == core)
    own_head = z - LOCAL * core
    my_pair = lax.div(z, 2)

    def slot(ref, j):
        return ref.at[:, pl.ds(pl.multiple_of((LOCAL - 1 - j) * ROWS, ROWS), ROWS)]

    def start(src, dst, s, r, to_sp, to_tp):
        remote(src, dst, s, r, to_sp, to_tp).start()

    def recv(dst, s, r):
        remote(dst, dst, s, r, sp, mate).wait_recv()

    def sent(src, s, r):
        remote(src, src, s, r, sp, mate).wait_send()

    def leaves(h):
        return jnp.logical_not(jnp.logical_and(keep, own_head == h))

    for h in range(LOCAL):
        @pl.when(leaves(h))
        def _(h=h):
            start(q_ref.at[h], slot(mine_ref, my_pair), qz_send.at[h], qz_recv.at[my_pair],
                  (LOCAL * core + h) * NX + x, 2 * y + to_core)
    for h in range(LOCAL):
        @pl.when(leaves(h))
        def _(h=h):
            start(kv_ref.at[h], all_ref.at[sp], kz_send.at[h], kz_recv.at[my_pair],
                  (LOCAL * core + h) * NX + x, 2 * y + to_core)
    for h in range(LOCAL):
        @pl.when(jnp.logical_not(leaves(h)))
        def _(h=h):
            all_ref[sp] = kv_ref[h]
            mine_ref[:, pl.ds(pl.multiple_of((LOCAL - 1 - my_pair) * ROWS, ROWS), ROWS)] = q_ref[h]

    def rows_of(ref, index, count, first=0):
        return ref.at[pl.ds(pl.multiple_of(index, count) + first, count)]

    wa_rows, wc_rows = LOCAL * VDIM, convs.shape[0] // n_tp
    width = wcol.shape[1]

    def columns(ref, owner_tp):
        return ref.at[:, pl.ds(pl.multiple_of(owner_tp * width, width), width)]

    def conv_part(owner_tp, first=0, count=wc_rows):
        return convs.at[pl.ds(pl.multiple_of(owner_tp * wc_rows + first, 16), count)]

    start(conv_ref, conv_part(tp), cy_send.at[0], cy_recv.at[0], sp, up)
    start(conv_ref, conv_part(tp), cy_send.at[1], cy_recv.at[1], sp, down)
    start(conv_ref, conv_part(tp), cd_send.at[0], cd_recv.at[0], sp, mate)
    for k in range(1, n_tp):
        to = lax.rem(tp + k, n_tp)
        start(columns(wa_ref, to), rows_of(wcol, tp * wa_rows, wa_rows), wa_send.at[k], wa_recv.at[k], sp, to)
        start(columns(wc_ref, to), rows_of(wconv, tp * wc_rows, wc_rows), wc_send.at[k], wc_recv.at[k], sp, to)
    own_wa = pltpu.make_async_copy(columns(wa_ref, tp), rows_of(wcol, tp * wa_rows, wa_rows), wa_send.at[0])
    own_wc = pltpu.make_async_copy(columns(wc_ref, tp), rows_of(wconv, tp * wc_rows, wc_rows), wc_send.at[0])
    own_wa.start()
    own_wc.start()
    convs[pl.ds(pl.multiple_of(tp * wc_rows, wc_rows), wc_rows), :] = conv_ref[...]

    m_ref[...] = jnp.full_like(m_ref, NEGATIVE)
    l_ref[...] = jnp.zeros_like(l_ref)
    acc_ref[...] = jnp.zeros_like(acc_ref)

    def z_wait(j, dst, s, r):
        @pl.when(jnp.logical_not(jnp.logical_and(keep, plane(j, core) == z)))
        def _():
            recv(dst, s, r)

    def stage_a(p):
        @pl.when(side(p) == core)
        def _():
            j = lax.div(p, 2)
            block = all_ref.at[p * NX + x]
            z_wait(j, block, kz_send.at[0], kz_recv.at[j])
            start(block, block, x_send.at[j, 0], x_recv.at[j, 0], z * NX + xp, tp)
            start(block, block, x_send.at[j, 1], x_recv.at[j, 1], z * NX + xm, tp)
            start(block, block, d_send.at[j, 0], d_recv.at[j, 0], sp, mate)

    def stage_b(p):
        @pl.when(side(p) == core)
        def _():
            j = lax.div(p, 2)
            low, high = all_ref.at[p * NX + xm], all_ref.at[p * NX + xp]
            recv(low, x_send.at[j, 0], x_recv.at[j, 0])
            part = all_ref.at[p * NX + xm, pl.ds(0, half)]
            start(part, part, x_send.at[j, 2], x_recv.at[j, 2], z * NX + xp, tp)
            start(low, low, d_send.at[j, 1], d_recv.at[j, 1], sp, mate)
            recv(high, x_send.at[j, 1], x_recv.at[j, 1])
            part = all_ref.at[p * NX + xp, pl.ds(half, half)]
            start(part, part, x_send.at[j, 3], x_recv.at[j, 3], z * NX + xm, tp)
            start(high, high, d_send.at[j, 2], d_recv.at[j, 2], sp, mate)

    def stage_c(p):
        j = lax.div(p, 2)
        parts = [all_ref.at[p * NX + xf, pl.ds(k * half, half)] for k in (0, 1)]

        @pl.when(side(p) == core)
        def _():
            for k in (0, 1):
                recv(parts[k], x_send.at[j, 2 + k], x_recv.at[j, 2 + k])
                start(parts[k], parts[k], d_send.at[j, 3 + k], d_recv.at[j, 3 + k], sp, mate)

        @pl.when(side(p) != core)
        def _():
            for k, column in enumerate((x, xm, xp)):
                recv(all_ref.at[p * NX + column], d_send.at[j, k], d_recv.at[j, k])
            for k in (0, 1):
                recv(parts[k], d_send.at[j, 3 + k], d_recv.at[j, 3 + k])

    def plane_at(i):
        step = lax.div(i + 1, 2)
        return lax.rem(z + jnp.where(lax.rem(i, 2) == 1, step, NZ - step), NZ)

    stage_a(plane_at(jnp.int32(0)))
    stage_a(plane_at(jnp.int32(1)))
    stage_b(plane_at(jnp.int32(0)))
    for j in range(LOCAL):
        z_wait(j, slot(mine_ref, j), qz_send.at[0], qz_recv.at[j])

    def ring_middle(part, y_s, y_r, d_s, d_r, rows):
        cut = rows // 2
        recv(part(down, 0, rows), y_s(0), y_r(0))
        start(part(down, 0, cut), part(down, 0, cut), y_s(2), y_r(2), sp, up)
        start(part(down, 0, rows), part(down, 0, rows), d_s(1), d_r(1), sp, mate)
        recv(part(up, 0, rows), y_s(1), y_r(1))
        start(part(up, cut, cut), part(up, cut, cut), y_s(3), y_r(3), sp, down)
        start(part(up, 0, rows), part(up, 0, rows), d_s(2), d_r(2), sp, mate)

    def ring_end(part, y_s, y_r, d_s, d_r, rows):
        cut = rows // 2
        for k in (0, 1):
            recv(part(far, k * cut, cut), y_s(2 + k), y_r(2 + k))
            start(part(far, k * cut, cut), part(far, k * cut, cut), d_s(3 + k), d_r(3 + k), sp, mate)

    def ring_recv(part, d_s, d_r, rows):
        cut = rows // 2
        recv(part(mate, 0, rows), d_s(0), d_r(0))
        recv(part(down + flip, 0, rows), d_s(1), d_r(1))
        recv(part(up + flip, 0, rows), d_s(2), d_r(2))
        for k in (0, 1):
            recv(part(far + flip, k * cut, cut), d_s(3 + k), d_r(3 + k))

    def ring_sent(part, y_s, y_r, d_s, d_r, rows):
        cut = rows // 2
        for k in (0, 1):
            sent(part(tp, 0, rows), y_s(k), y_r(k))
            sent(part(tp, 0, cut), y_s(2 + k), y_r(2 + k))
            sent(part(tp, 0, cut), d_s(3 + k), d_r(3 + k))
        for k in (0, 1, 2):
            sent(part(tp, 0, rows), d_s(k), d_r(k))

    conv_sems = [lambda k, ref=ref: ref.at[k] for ref in (cy_send, cy_recv, cd_send, cd_recv)]
    ring_middle(conv_part, *conv_sems, wc_rows)
    ring_end(conv_part, *conv_sems, wc_rows)

    def work(i, carry):
        @pl.when(i + 2 < NZ)
        def _():
            stage_a(plane_at(i + 2))

        @pl.when(i + 1 < NZ)
        def _():
            stage_b(plane_at(i + 1))

        p = plane_at(i)
        stage_c(p)
        attend_plane(all_ref, mine_ref, (m_ref, l_ref, acc_ref), p, core, x)
        return carry

    lax.fori_loop(0, NZ, work, 0)

    total = m_ref[...] * (1.0 / LOG2E) + jnp.log(l_ref[...])
    scaled = acc_ref[...] * (1.0 / l_ref[...])
    to = 2 * y + owner

    def head_rows(owner_tp, h, first=0, count=VDIM):
        return heads.at[pl.ds(pl.multiple_of((owner_tp * LOCAL + h) * VDIM + first, 16), count)]

    head = lax.rem(z, LOCAL)
    for j in range(LOCAL):
        cols = slice((LOCAL - 1 - j) * ROWS, (LOCAL - j) * ROWS)
        results[j] = scaled[:, cols].astype(jnp.bfloat16)
        logs[j] = jnp.broadcast_to(total[:, cols], logs.shape[1:])

    def stays(j):
        return jnp.logical_and(keep, plane(j, core) == z)

    for j in range(LOCAL):
        @pl.when(jnp.logical_not(stays(j)))
        def _(j=j):
            start(results.at[j], head_rows(to, head), rz_send.at[j], rz_recv.at[head], plane(j, core) * NX + x, to)
            start(logs.at[j], logs_ref.at[head], lz_send.at[j], lz_recv.at[head], plane(j, core) * NX + x, to)
    for j in range(LOCAL):
        @pl.when(stays(j))
        def _(j=j):
            heads[pl.ds(pl.multiple_of((to * LOCAL + head) * VDIM, VDIM), VDIM), :] = results[j]
            logs_ref[head] = logs[j]

    ring_recv(conv_part, conv_sems[2], conv_sems[3], wc_rows)
    own_wc.wait()
    own_wa.wait()
    for k in range(1, n_tp):
        source = lax.rem(tp + n_tp - k, n_tp)
        recv(rows_of(wconv, source * wc_rows, wc_rows), wc_send.at[k], wc_recv.at[k])
        recv(rows_of(wcol, source * wa_rows, wa_rows), wa_send.at[k], wa_recv.at[k])
    turned = (((0,), (0,)), ((), ()))
    projected = lax.dot_general(convs[...], wconv[...], turned, preferred_element_type=jnp.float32)

    def here(h):
        return jnp.logical_and(keep, LOCAL * core + h == z)

    def head_ring(h):
        return (
            lambda owner_tp, first, count: head_rows(owner_tp, h, first, count),
            *[lambda k, ref=ref: ref.at[h, k] for ref in (hy_send, hy_recv, hd_send, hd_recv)],
            VDIM,
        )

    for step in range(LOCAL + 2):
        if step < LOCAL:
            h = step
            mine = head_rows(tp, h)

            @pl.when(jnp.logical_not(here(h)))
            def _(h=h, mine=mine):
                recv(mine, rz_send.at[h], rz_recv.at[h])

            start(mine, mine, hy_send.at[h, 0], hy_recv.at[h, 0], sp, up)
            start(mine, mine, hy_send.at[h, 1], hy_recv.at[h, 1], sp, down)
            start(mine, mine, hd_send.at[h, 0], hd_recv.at[h, 0], sp, mate)
        if 1 <= step <= LOCAL:
            ring_middle(*head_ring(step - 1))
        if step >= 2:
            ring_end(*head_ring(step - 2))
    for h in range(LOCAL):
        part, _, _, d_s, d_r, rows = head_ring(h)
        ring_recv(part, d_s, d_r, rows)
    projected = projected + lax.dot_general(heads[...], wcol[...], turned, preferred_element_type=jnp.float32)

    squares = projected * projected
    lanes = width // 2
    column = jnp.sum((squares[:, :lanes] + squares[:, lanes:]).T, axis=0, keepdims=True)
    stats[tp] = jnp.broadcast_to(column, stats.shape[1:])
    for k in range(1, n_tp):
        start(stats.at[tp], stats.at[tp], s_send.at[k], s_recv.at[k], sp, lax.rem(tp + k, n_tp))
    for k in range(1, n_tp):
        recv(stats.at[lax.rem(tp + n_tp - k, n_tp)], s_send.at[k], s_recv.at[k])
    summed = functools.reduce(jnp.add, [stats[t, 0:1, :] for t in range(n_tp)])
    norm = lax.rsqrt(summed * (1.0 / D) + EPSILON)
    norm = jnp.broadcast_to(norm, (lanes, ROWS)).T
    for k in (0, 1):
        cols = slice(k * lanes, (k + 1) * lanes)
        mixed_ref[:, cols] = (projected[:, cols] * norm * gain_ref[:, cols]).astype(jnp.bfloat16)

    for h in range(LOCAL):
        @pl.when(leaves(h))
        def _(h=h):
            sent(q_ref.at[h], qz_send.at[h], qz_recv.at[h])
            sent(kv_ref.at[h], kz_send.at[h], kz_recv.at[h])
    for j in range(LOCAL):
        block = all_ref.at[0]
        part = all_ref.at[0, pl.ds(0, half)]
        for k in (0, 1):
            sent(block, x_send.at[j, k], x_recv.at[j, k])
            sent(part, x_send.at[j, 2 + k], x_recv.at[j, 2 + k])
            sent(part, d_send.at[j, 3 + k], d_recv.at[j, 3 + k])
        for k in (0, 1, 2):
            sent(block, d_send.at[j, k], d_recv.at[j, k])

        @pl.when(jnp.logical_not(stays(j)))
        def _(j=j):
            sent(results.at[j], rz_send.at[j], rz_recv.at[j])
            sent(logs.at[j], lz_send.at[j], lz_recv.at[j])

        @pl.when(jnp.logical_not(here(j)))
        def _(j=j):
            recv(logs_ref.at[j], lz_send.at[j], lz_recv.at[j])

        ring_sent(*head_ring(j))
    ring_sent(conv_part, *conv_sems, wc_rows)
    for k in range(1, n_tp):
        sent(rows_of(wcol, 0, wa_rows), wa_send.at[k], wa_recv.at[k])
        sent(rows_of(wconv, 0, wc_rows), wc_send.at[k], wc_recv.at[k])
        sent(stats.at[0], s_send.at[k], s_recv.at[k])


def layer_rest(kv, q, conv, gain, wa, wc):
    dma = pltpu.SemaphoreType.DMA
    wa_rows, wc_rows = wa.shape[0], wc.shape[0]
    n_tp = 2 * NY
    width = wa.shape[1] // n_tp
    bf16, f32 = jnp.bfloat16, jnp.float32
    sems = []
    for shape in ((4,), (4,), (4, 4), (4, 5), (8,), (8,), (4,), (5,), (4,), (4,), (4, 4), (4, 5), (8,)):
        sems += [dma(shape), dma(shape)]
    return pl.pallas_call(
        layer_kernel,
        out_shape=(
            jax.ShapeDtypeStruct((ROWS, width), bf16),
            jax.ShapeDtypeStruct((LOCAL, 8, ROWS), f32),
        ),
        in_specs=[pl.BlockSpec(memory_space=VMEM)] * 4 + [pl.BlockSpec(memory_space=pl.ANY)] * 2,
        out_specs=(pl.BlockSpec(memory_space=VMEM),) * 2,
        scratch_shapes=[
            pltpu.VMEM((BLOCKS, KVR, ROWS), bf16),
            pltpu.VMEM((QK, LOCAL * ROWS), bf16),
            pltpu.VMEM((wa_rows * n_tp, width), bf16),
            pltpu.VMEM((wc_rows * n_tp, width), bf16),
            pltpu.VMEM((wc_rows * n_tp, ROWS), bf16),
            pltpu.VMEM((wa_rows * n_tp, ROWS), bf16),
            pltpu.VMEM((LOCAL, VDIM, ROWS), bf16),
            pltpu.VMEM((LOCAL, 8, ROWS), f32),
            pltpu.VMEM((n_tp, 8, ROWS), f32),
            pltpu.VMEM((1, LOCAL * ROWS), f32),
            pltpu.VMEM((1, LOCAL * ROWS), f32),
            pltpu.VMEM((VDIM, LOCAL * ROWS), f32),
        ] + sems,
        compiler_params=pltpu.CompilerParams(
            collective_id=1, has_side_effects=True, vmem_limit_bytes=56 * 2**20,
        ),
        name="layer_rest",
    )(kv, q, conv, gain, wa, wc)


def from_behind(value, axis, steps):
    count = lax.axis_size(axis)
    leading, last = (max(0, -steps), min(count, count - steps))
    return lax.ppermute(value, axis, [(source, source + steps) for source in range(leading, last)])


def rms_factor(values):
    return lax.rsqrt(jnp.mean(values * values, axis=-1, keepdims=True) + EPSILON)


def rotation(positions, width):
    freqs = THETA ** (-jnp.arange(0, width, 2, dtype=jnp.float32) / width)
    angles = freqs[:, None] * positions.astype(jnp.float32)[None, :]
    return (jnp.cos(angles), jnp.sin(angles))


def rotate(values, cosine, sine):
    half = values.shape[-2] // 2
    first = values[..., :half, :]
    second = values[..., half:, :]
    return jnp.concatenate(
        [first * cosine - second * sine, second * cosine + first * sine], axis=-2
    )


def dot_turned(weight, rows):
    return lax.dot_general(
        weight, rows, (((0,), (1,)), ((), ())), preferred_element_type=jnp.float32
    )


def body(
    tokens,
    pre_gain,
    outer_gate_weight,
    inner_gate_weight,
    source_weight,
    conv_taps,
    q_down_weight,
    q_norm_gain,
    q_up_weight,
    kv_down_weight,
    rope_key_weight,
    kv_norm_gain,
    kv_up_weight,
    attn_out_weight,
    conv_out_weight,
    post_gain,
):
    token_rows = tokens.shape[0]
    wide = gathered(tokens, 0).astype(jnp.float32)
    scaled = (wide * pre_gain).astype(jnp.bfloat16)
    squares = jnp.sum(wide * wide, axis=1)
    factor = lax.rsqrt(squares / D + EPSILON)[:, None]

    def project(weight):
        return jnp.dot(scaled, weight, preferred_element_type=jnp.float32) * factor

    query_pos = lax.axis_index("sp") * token_rows + jnp.arange(token_rows, dtype=jnp.int32)
    cosine, sine = rotation(query_pos, ROPE)
    q_latent = project(q_down_weight)
    q_normed = (q_latent * rms_factor(q_latent) * q_norm_gain).astype(jnp.bfloat16)
    query = dot_turned(q_up_weight, q_normed).reshape(LOCAL, QK, token_rows)
    q_send = jnp.concatenate(
        [query[:, :NOPE], rotate(query[:, NOPE:], cosine, sine)], axis=1
    ).astype(jnp.bfloat16)
    kv_latent = project(kv_down_weight)
    latent = (kv_latent * rms_factor(kv_latent) * kv_norm_gain).astype(jnp.bfloat16)
    rope_key = rotate(project(rope_key_weight).T, cosine, sine).astype(jnp.bfloat16)
    keyvals = dot_turned(kv_up_weight, latent).astype(jnp.bfloat16)
    keyvals = keyvals.reshape(LOCAL, NOPE + VDIM, token_rows)
    kv_send = jnp.concatenate(
        [
            keyvals[:, :NOPE],
            jnp.broadcast_to(rope_key[None], (LOCAL, ROPE, token_rows)),
            keyvals[:, NOPE:],
        ],
        axis=1,
    )

    def project_turned(weight):
        return dot_turned(weight, scaled) * factor[:, 0][None, :]

    outer = project_turned(outer_gate_weight).astype(jnp.bfloat16)
    inner = project_turned(inner_gate_weight).astype(jnp.bfloat16)
    source = project_turned(source_weight).astype(jnp.bfloat16)
    driven = (inner.astype(jnp.float32) * source.astype(jnp.float32)).astype(jnp.bfloat16)
    prior = from_behind(driven[:, token_rows - (TAPS - 1) :], "sp", 1)
    extended = jnp.concatenate([prior, driven], axis=1)
    convolved = jnp.zeros(driven.shape, jnp.float32)
    for index in range(TAPS):
        convolved = convolved + conv_taps[index].astype(jnp.float32)[:, None] * extended[
            :, index : index + token_rows
        ].astype(jnp.float32)
    conv_branch = (outer.astype(jnp.float32) * convolved).astype(jnp.bfloat16)

    mixed, logs = layer_rest(
        kv_send, q_send, conv_branch, post_gain[None, :], attn_out_weight, conv_out_weight
    )
    return (mixed, logs[:, 0, :])


def solution(mesh):
    placed = (
        P("sp", "tp"),
        P(),
        P(None, "tp"),
        P(None, "tp"),
        P(None, "tp"),
        P(None, "tp"),
        P(),
        P(),
        P(None, "tp"),
        P(),
        P(),
        P(),
        P(None, "tp"),
        P("tp", None),
        P("tp", None),
        P("tp"),
    )
    return jax.shard_map(
        body, mesh=mesh, in_specs=placed, out_specs=(P("sp", "tp"), P("tp", "sp")), check_vma=False
    )
```

```python
import functools
import math

import jax
import jax.numpy as jnp
from jax import lax
from jax.experimental import pallas as pl
from jax.experimental.pallas import tpu as pltpu
from jax.sharding import PartitionSpec as P

D = 2048
NOPE = 64
ROPE = 32
VDIM = 64
TAPS = 3
NZ, NX, NY = 8, 4, 4
ROWS = 384
KVR = NOPE + ROPE + VDIM
QK = NOPE + ROPE
LOCAL = 4
BLOCKS = NZ * NX

EPSILON = 1e-06
THETA = 500000.0
NEGATIVE = -1e30
LOG2E = math.log2(math.e)
MESH = pl.DeviceIdType.MESH
VMEM = pltpu.MemorySpace.VMEM


def side(z):
    return lax.rem(lax.div(z + 1, 2), 2)


def plane(j, core):
    return 2 * j + lax.rem(j + core, 2)


def remote(src, dst, send, recv, sp, tp):
    return pltpu.make_async_remote_copy(
        src_ref=src, dst_ref=dst, send_sem=send, recv_sem=recv,
        device_id=(sp, tp), device_id_type=MESH,
    )


def attention_step(kv_ref, q_ref, m_ref, l_ref, acc_ref, block, group, active, offset):
    scale = QK ** -0.5 * LOG2E
    width = active * ROWS
    cols = slice(0, width)
    scores = []
    for g in range(group):
        keys = kv_ref[block + g, 0:QK, :].T
        value = jnp.dot(keys, q_ref[:, cols], preferred_element_type=jnp.float32)
        if offset is not None:
            start = width - ROWS
            key = lax.broadcasted_iota(jnp.int32, value.shape, 0) + (offset + g * ROWS)
            row = lax.broadcasted_iota(jnp.int32, value.shape, 1) - start
            keep = key <= row
            if start:
                keep = jnp.logical_or(keep, row < 0)
            value = jnp.where(keep, value, NEGATIVE)
        scores.append(value)
    old = m_ref[:, cols]
    top = functools.reduce(jnp.maximum, [jnp.max(v, axis=0, keepdims=True) for v in scores])
    fresh = jnp.maximum(old, top * scale)
    shrink = jnp.exp2(old - fresh)
    weights = [jnp.exp2(v * scale - fresh) for v in scores]
    m_ref[:, cols] = fresh
    l_ref[:, cols] = l_ref[:, cols] * shrink + sum(
        jnp.sum(w, axis=0, keepdims=True) for w in weights
    )
    acc_ref[:, cols] = acc_ref[:, cols] * shrink + sum(
        jnp.dot(kv_ref[block + g, QK:KVR, :], w.astype(jnp.bfloat16), preferred_element_type=jnp.float32)
        for g, w in enumerate(weights)
    )


GROUPS = {4: 1, 3: 1, 2: 2, 1: 4}


def attend_plane(kv_ref, q_ref, state, p, core, x):
    direct = side(p) == core
    pair = lax.div(p, 2)
    later = LOCAL - pair - lax.rem(p, 2)
    for active in range(1, LOCAL + 1):
        group = GROUPS[active]

        @pl.when(jnp.logical_and(direct, pair == LOCAL - active))
        def _(active=active, group=group):
            def advance(i, carry):
                attention_step(kv_ref, q_ref, *state, p * NX + i * group, group, active,
                               (i * group - x) * ROWS)
                return carry

            lax.fori_loop(0, NX // group, advance, 0)

        @pl.when(jnp.logical_and(jnp.logical_not(direct), later == active))
        def _(active=active, group=group):
            def advance(i, carry):
                attention_step(kv_ref, q_ref, *state, p * NX + i * group, group, active, None)
                return carry

            lax.fori_loop(0, NX // group, advance, 0)


def layer_kernel(
    tokens_ref, pre_ref, taps_ref, qgain_ref, kvgain_ref, gain_ref, rope_ref, cos_ref, sin_ref,
    wo_ref, wi_ref, ws_ref, wq_ref, wkv_ref, wqup_ref, wkvup_ref, wa_ref, wc_ref,
    mixed_ref, logs_ref,
    tok, wall, wqup, wkvup, sums, squares, driven, kv_ref, q_ref, conv_ref,
    all_ref, mine_ref, wcol, wconv, convs, heads, results, logs, stats, m_ref, l_ref, acc_ref,
    load_sem, halo_send, halo_recv, ty_send, ty_recv, td_send, td_recv,
    kz_send, kz_recv, qz_send, qz_recv, x_send, x_recv, d_send, d_recv,
    wa_send, wa_recv, wc_send, wc_recv, cy_send, cy_recv, cd_send, cd_recv,
    rz_send, rz_recv, lz_send, lz_recv, hy_send, hy_recv, hd_send, hd_recv, s_send, s_recv,
):
    sp = lax.axis_index("sp")
    tp = lax.axis_index("tp")
    z, x = lax.div(sp, NX), lax.rem(sp, NX)
    core, y = lax.rem(tp, 2), lax.div(tp, 2)
    other = 1 - core
    mate = tp + 1 - 2 * core
    xp, xm, xf = (lax.rem(x + k, NX) for k in (1, NX - 1, 2))
    up, down, far = (lax.rem(y + k, NY) * 2 + core for k in (1, NY - 1, 2))
    flip = other - core
    to_core = side(z)
    owner = lax.div(z, LOCAL)
    half = KVR // 2
    n_tp = 2 * NY

    peers = [(lax.rem(z + k, NZ) * NX + x, 2 * y + c) for k in range(1, NZ) for c in (0, 1)]
    peers += [(z * NX + xp, tp), (z * NX + xm, tp)]
    peers += [(lax.rem(sp + k, BLOCKS), tp) for k in (1, BLOCKS - 1)]
    peers += [(sp, lax.rem(tp + k, n_tp)) for k in range(1, n_tp)]

    edges = [0]
    for ref in (wkv_ref, wq_ref, wo_ref, wi_ref, ws_ref):
        edges.append(edges[-1] + ref.shape[1])
    loads = [
        pltpu.make_async_copy(ref, wall.at[:, pl.ds(edges[i], ref.shape[1])], load_sem.at[i])
        for i, ref in enumerate((wkv_ref, wq_ref, wo_ref, wi_ref, ws_ref))
    ]
    loads += [
        pltpu.make_async_copy(wkvup_ref, wkvup, load_sem.at[5]),
        pltpu.make_async_copy(wqup_ref, wqup, load_sem.at[6]),
    ]
    for c in loads:
        c.start()
    barrier = pltpu.get_barrier_semaphore()
    for peer in peers:
        pl.semaphore_signal(barrier, inc=1, device_id=peer, device_id_type=MESH)
    pad = jnp.zeros((128 - ROPE, rope_ref.shape[1]), jnp.float32)
    wall[:, pl.ds(edges[-1], 128)] = (
        jnp.concatenate([rope_ref[...].astype(jnp.float32), pad], axis=0).T.astype(jnp.bfloat16)
    )
    pl.semaphore_wait(barrier, len(peers))

    keep = jnp.logical_and(owner == core, to_core == core)
    own_head = z - LOCAL * core
    my_pair = lax.div(z, 2)

    def slot(ref, j):
        return ref.at[:, pl.ds(pl.multiple_of((LOCAL - 1 - j) * ROWS, ROWS), ROWS)]

    def start(src, dst, s, r, to_sp, to_tp):
        remote(src, dst, s, r, to_sp, to_tp).start()

    def recv(dst, s, r):
        remote(dst, dst, s, r, sp, mate).wait_recv()

    def sent(src, s, r):
        remote(src, src, s, r, sp, mate).wait_send()

    def leaves(h):
        return jnp.logical_not(jnp.logical_and(keep, own_head == h))

    def ring_start(source, part, y_s, y_r, d_s, d_r, rows):
        start(source, part(tp, 0, rows), y_s(0), y_r(0), sp, up)
        start(source, part(tp, 0, rows), y_s(1), y_r(1), sp, down)
        start(source, part(tp, 0, rows), d_s(0), d_r(0), sp, mate)

    def ring_middle(part, y_s, y_r, d_s, d_r, rows):
        cut = rows // 2
        recv(part(down, 0, rows), y_s(0), y_r(0))
        start(part(down, 0, cut), part(down, 0, cut), y_s(2), y_r(2), sp, up)
        start(part(down, 0, rows), part(down, 0, rows), d_s(1), d_r(1), sp, mate)
        recv(part(up, 0, rows), y_s(1), y_r(1))
        start(part(up, cut, cut), part(up, cut, cut), y_s(3), y_r(3), sp, down)
        start(part(up, 0, rows), part(up, 0, rows), d_s(2), d_r(2), sp, mate)

    def ring_end(part, y_s, y_r, d_s, d_r, rows):
        cut = rows // 2
        for k in (0, 1):
            recv(part(far, k * cut, cut), y_s(2 + k), y_r(2 + k))
            start(part(far, k * cut, cut), part(far, k * cut, cut), d_s(3 + k), d_r(3 + k), sp, mate)

    def ring_far(part, d_s, d_r, rows):
        cut = rows // 2
        for k in (0, 1):
            recv(part(far + flip, k * cut, cut), d_s(3 + k), d_r(3 + k))

    def ring_recv(part, d_s, d_r, rows):
        recv(part(mate, 0, rows), d_s(0), d_r(0))
        recv(part(down + flip, 0, rows), d_s(1), d_r(1))
        recv(part(up + flip, 0, rows), d_s(2), d_r(2))
        ring_far(part, d_s, d_r, rows)

    def ring_sent(part, y_s, y_r, d_s, d_r, rows):
        cut = rows // 2
        for k in (0, 1):
            sent(part(tp, 0, rows), y_s(k), y_r(k))
            sent(part(tp, 0, cut), y_s(2 + k), y_r(2 + k))
            sent(part(tp, 0, cut), d_s(3 + k), d_r(3 + k))
        for k in (0, 1, 2):
            sent(part(tp, 0, rows), d_s(k), d_r(k))

    part_width = tokens_ref.shape[1]

    def token_part(owner_tp, first=0, count=ROWS):
        return tok.at[pl.ds(first, count), pl.ds(pl.multiple_of(owner_tp * part_width, part_width), part_width)]

    tok_sems = [lambda k, ref=ref: ref.at[k] for ref in (ty_send, ty_recv, td_send, td_recv)]
    ring_start(tokens_ref, token_part, *tok_sems, ROWS)
    tok[:, pl.ds(pl.multiple_of(tp * part_width, part_width), part_width)] = tokens_ref[...]

    def project(chip, fresh):
        share = 2 * part_width
        cols = pl.ds(pl.multiple_of(chip * share, share), share)
        wide = tok[:, cols].astype(jnp.float32)
        part = wide * wide
        part = functools.reduce(jnp.add, [part[:, k : k + 128] for k in range(0, share, 128)])
        value = jnp.dot((wide * pre_ref[:, cols]).astype(jnp.bfloat16), wall[cols, :],
                        preferred_element_type=jnp.float32)
        squares[...] = part if fresh else squares[...] + part
        sums[...] = value if fresh else sums[...] + value

    recv(token_part(mate), td_send.at[0], td_recv.at[0])
    for c in loads[:5]:
        c.wait()
    project(y, True)
    ring_middle(token_part, *tok_sems, ROWS)
    recv(token_part(down + flip), td_send.at[1], td_recv.at[1])
    project(lax.div(down, 2), False)
    ring_end(token_part, *tok_sems, ROWS)
    recv(token_part(up + flip), td_send.at[2], td_recv.at[2])
    project(lax.div(up, 2), False)
    ring_far(token_part, tok_sems[2], tok_sems[3], ROWS)
    project(lax.div(far, 2), False)
    factor = lax.rsqrt(jnp.sum(squares[...], axis=1, keepdims=True) * (1.0 / D) + EPSILON)

    def normed(first, last, gain):
        value = sums[:, first:last] * factor
        mean = jnp.sum(value * value, axis=1, keepdims=True) * (1.0 / (last - first))
        return (value * lax.rsqrt(mean + EPSILON) * gain).astype(jnp.bfloat16)

    cosine, sine = cos_ref[...], sin_ref[...]

    def rotate(first, second):
        return jnp.concatenate(
            [first * cosine - second * sine, second * cosine + first * sine], axis=0
        ).astype(jnp.bfloat16)

    loads[5].wait()
    keyvals = jnp.dot(normed(edges[0], edges[1], kvgain_ref[...]), wkvup[...], preferred_element_type=jnp.float32).T
    turn = (sums[:, edges[-1] : edges[-1] + 128] * factor).T
    rope_key = rotate(turn[: ROPE // 2], turn[ROPE // 2 : ROPE])
    for h in range(LOCAL):
        first = h * (NOPE + VDIM)
        kv_ref[h, 0:NOPE] = keyvals[first : first + NOPE].astype(jnp.bfloat16)
        kv_ref[h, NOPE:QK] = rope_key
        kv_ref[h, QK:KVR] = keyvals[first + NOPE : first + NOPE + VDIM].astype(jnp.bfloat16)
    for h in range(LOCAL):
        @pl.when(leaves(h))
        def _(h=h):
            start(kv_ref.at[h], all_ref.at[sp], kz_send.at[h], kz_recv.at[my_pair],
                  (LOCAL * core + h) * NX + x, 2 * y + to_core)

        @pl.when(jnp.logical_not(leaves(h)))
        def _(h=h):
            all_ref[sp] = kv_ref[h]

    loads[6].wait()
    query = jnp.dot(normed(edges[1], edges[2], qgain_ref[...]), wqup[...], preferred_element_type=jnp.float32).T
    for h in range(LOCAL):
        first = h * QK
        q_ref[h, 0:NOPE] = query[first : first + NOPE].astype(jnp.bfloat16)
        q_ref[h, NOPE:QK] = rotate(query[first + NOPE : first + NOPE + ROPE // 2],
                                   query[first + NOPE + ROPE // 2 : first + QK])
    for h in range(LOCAL):
        @pl.when(leaves(h))
        def _(h=h):
            start(q_ref.at[h], slot(mine_ref, my_pair), qz_send.at[h], qz_recv.at[my_pair],
                  (LOCAL * core + h) * NX + x, 2 * y + to_core)

        @pl.when(jnp.logical_not(leaves(h)))
        def _(h=h):
            mine_ref[:, pl.ds(pl.multiple_of((LOCAL - 1 - my_pair) * ROWS, ROWS), ROWS)] = q_ref[h]

    outer, inner, source = (
        (sums[:, edges[k] : edges[k + 1]] * factor).astype(jnp.bfloat16) for k in (2, 3, 4)
    )
    driven[pl.ds(16, ROWS), :] = (inner.astype(jnp.float32) * source.astype(jnp.float32)).astype(jnp.bfloat16)

    @pl.when(sp < BLOCKS - 1)
    def _():
        start(driven.at[pl.ds(ROWS + 8, 8)], driven.at[pl.ds(8, 8)], halo_send, halo_recv, sp + 1, tp)

    @pl.when(sp == 0)
    def _():
        driven[pl.ds(8, 8), :] = jnp.zeros((8, driven.shape[1]), jnp.bfloat16)

    @pl.when(sp > 0)
    def _():
        recv(driven.at[pl.ds(8, 8)], halo_send, halo_recv)

    extended = driven[pl.ds(8, ROWS + 8), :].astype(jnp.float32)
    taps = taps_ref[...].astype(jnp.float32)
    convolved = functools.reduce(
        jnp.add,
        [taps[k : k + 1] * extended[9 - TAPS + k : 9 - TAPS + k + ROWS] for k in range(TAPS)],
    )
    conv_ref[...] = (outer.astype(jnp.float32) * convolved).T.astype(jnp.bfloat16)

    def rows_of(ref, index, count, first=0):
        return ref.at[pl.ds(pl.multiple_of(index, count) + first, count)]

    wa_rows, wc_rows = LOCAL * VDIM, convs.shape[0] // n_tp
    width = wcol.shape[1]

    def columns(ref, owner_tp):
        return ref.at[:, pl.ds(pl.multiple_of(owner_tp * width, width), width)]

    def conv_part(owner_tp, first=0, count=wc_rows):
        return convs.at[pl.ds(pl.multiple_of(owner_tp * wc_rows + first, 16), count)]

    conv_sems = [lambda k, ref=ref: ref.at[k] for ref in (cy_send, cy_recv, cd_send, cd_recv)]
    ring_start(conv_ref, conv_part, *conv_sems, wc_rows)
    for k in range(1, n_tp):
        to = lax.rem(tp + k, n_tp)
        start(columns(wa_ref, to), rows_of(wcol, tp * wa_rows, wa_rows), wa_send.at[k], wa_recv.at[k], sp, to)
        start(columns(wc_ref, to), rows_of(wconv, tp * wc_rows, wc_rows), wc_send.at[k], wc_recv.at[k], sp, to)
    own_wa = pltpu.make_async_copy(columns(wa_ref, tp), rows_of(wcol, tp * wa_rows, wa_rows), wa_send.at[0])
    own_wc = pltpu.make_async_copy(columns(wc_ref, tp), rows_of(wconv, tp * wc_rows, wc_rows), wc_send.at[0])
    own_wa.start()
    own_wc.start()
    convs[pl.ds(pl.multiple_of(tp * wc_rows, wc_rows), wc_rows), :] = conv_ref[...]

    m_ref[...] = jnp.full_like(m_ref, NEGATIVE)
    l_ref[...] = jnp.zeros_like(l_ref)
    acc_ref[...] = jnp.zeros_like(acc_ref)

    def z_wait(j, dst, s, r):
        @pl.when(jnp.logical_not(jnp.logical_and(keep, plane(j, core) == z)))
        def _():
            recv(dst, s, r)

    def stage_a(p):
        @pl.when(side(p) == core)
        def _():
            j = lax.div(p, 2)
            block = all_ref.at[p * NX + x]
            z_wait(j, block, kz_send.at[0], kz_recv.at[j])
            start(block, block, x_send.at[j, 0], x_recv.at[j, 0], z * NX + xp, tp)
            start(block, block, x_send.at[j, 1], x_recv.at[j, 1], z * NX + xm, tp)
            start(block, block, d_send.at[j, 0], d_recv.at[j, 0], sp, mate)

    def stage_b(p):
        @pl.when(side(p) == core)
        def _():
            j = lax.div(p, 2)
            low, high = all_ref.at[p * NX + xm], all_ref.at[p * NX + xp]
            recv(low, x_send.at[j, 0], x_recv.at[j, 0])
            part = all_ref.at[p * NX + xm, pl.ds(0, half)]
            start(part, part, x_send.at[j, 2], x_recv.at[j, 2], z * NX + xp, tp)
            start(low, low, d_send.at[j, 1], d_recv.at[j, 1], sp, mate)
            recv(high, x_send.at[j, 1], x_recv.at[j, 1])
            part = all_ref.at[p * NX + xp, pl.ds(half, half)]
            start(part, part, x_send.at[j, 3], x_recv.at[j, 3], z * NX + xm, tp)
            start(high, high, d_send.at[j, 2], d_recv.at[j, 2], sp, mate)

    def stage_c(p):
        j = lax.div(p, 2)
        parts = [all_ref.at[p * NX + xf, pl.ds(k * half, half)] for k in (0, 1)]

        @pl.when(side(p) == core)
        def _():
            for k in (0, 1):
                recv(parts[k], x_send.at[j, 2 + k], x_recv.at[j, 2 + k])
                start(parts[k], parts[k], d_send.at[j, 3 + k], d_recv.at[j, 3 + k], sp, mate)

        @pl.when(side(p) != core)
        def _():
            for k, column in enumerate((x, xm, xp)):
                recv(all_ref.at[p * NX + column], d_send.at[j, k], d_recv.at[j, k])
            for k in (0, 1):
                recv(parts[k], d_send.at[j, 3 + k], d_recv.at[j, 3 + k])

    def plane_at(i):
        step = lax.div(i + 1, 2)
        return lax.rem(z + jnp.where(lax.rem(i, 2) == 1, step, NZ - step), NZ)

    stage_a(plane_at(jnp.int32(0)))
    stage_a(plane_at(jnp.int32(1)))
    stage_b(plane_at(jnp.int32(0)))
    for j in range(LOCAL):
        z_wait(j, slot(mine_ref, j), qz_send.at[0], qz_recv.at[j])

    ring_middle(conv_part, *conv_sems, wc_rows)
    ring_end(conv_part, *conv_sems, wc_rows)

    def work(i, carry):
        @pl.when(i + 2 < NZ)
        def _():
            stage_a(plane_at(i + 2))

        @pl.when(i + 1 < NZ)
        def _():
            stage_b(plane_at(i + 1))

        p = plane_at(i)
        stage_c(p)
        attend_plane(all_ref, mine_ref, (m_ref, l_ref, acc_ref), p, core, x)
        return carry

    lax.fori_loop(0, NZ, work, 0)

    total = m_ref[...] * (1.0 / LOG2E) + jnp.log(l_ref[...])
    scaled = acc_ref[...] * (1.0 / l_ref[...])
    to = 2 * y + owner

    def head_rows(owner_tp, h, first=0, count=VDIM):
        return heads.at[pl.ds(pl.multiple_of((owner_tp * LOCAL + h) * VDIM + first, 16), count)]

    head = lax.rem(z, LOCAL)
    for j in range(LOCAL):
        cols = slice((LOCAL - 1 - j) * ROWS, (LOCAL - j) * ROWS)
        results[j] = scaled[:, cols].astype(jnp.bfloat16)
        logs[j] = jnp.broadcast_to(total[:, cols], logs.shape[1:])

    def stays(j):
        return jnp.logical_and(keep, plane(j, core) == z)

    for j in range(LOCAL):
        @pl.when(jnp.logical_not(stays(j)))
        def _(j=j):
            start(results.at[j], head_rows(to, head), rz_send.at[j], rz_recv.at[head], plane(j, core) * NX + x, to)
            start(logs.at[j], logs_ref.at[head], lz_send.at[j], lz_recv.at[head], plane(j, core) * NX + x, to)
    for j in range(LOCAL):
        @pl.when(stays(j))
        def _(j=j):
            heads[pl.ds(pl.multiple_of((to * LOCAL + head) * VDIM, VDIM), VDIM), :] = results[j]
            logs_ref[head] = logs[j]

    ring_recv(conv_part, conv_sems[2], conv_sems[3], wc_rows)
    own_wc.wait()
    own_wa.wait()
    for k in range(1, n_tp):
        source = lax.rem(tp + n_tp - k, n_tp)
        recv(rows_of(wconv, source * wc_rows, wc_rows), wc_send.at[k], wc_recv.at[k])
        recv(rows_of(wcol, source * wa_rows, wa_rows), wa_send.at[k], wa_recv.at[k])
    turned = (((0,), (0,)), ((), ()))
    projected = lax.dot_general(convs[...], wconv[...], turned, preferred_element_type=jnp.float32)

    def here(h):
        return jnp.logical_and(keep, LOCAL * core + h == z)

    def head_ring(h):
        return (
            lambda owner_tp, first, count: head_rows(owner_tp, h, first, count),
            *[lambda k, ref=ref: ref.at[h, k] for ref in (hy_send, hy_recv, hd_send, hd_recv)],
            VDIM,
        )

    for step in range(LOCAL + 2):
        if step < LOCAL:
            h = step
            mine = head_rows(tp, h)

            @pl.when(jnp.logical_not(here(h)))
            def _(h=h, mine=mine):
                recv(mine, rz_send.at[h], rz_recv.at[h])

            start(mine, mine, hy_send.at[h, 0], hy_recv.at[h, 0], sp, up)
            start(mine, mine, hy_send.at[h, 1], hy_recv.at[h, 1], sp, down)
            start(mine, mine, hd_send.at[h, 0], hd_recv.at[h, 0], sp, mate)
        if 1 <= step <= LOCAL:
            ring_middle(*head_ring(step - 1))
        if step >= 2:
            ring_end(*head_ring(step - 2))
    for h in range(LOCAL):
        part, _, _, d_s, d_r, rows = head_ring(h)
        ring_recv(part, d_s, d_r, rows)
    projected = projected + lax.dot_general(heads[...], wcol[...], turned, preferred_element_type=jnp.float32)

    squares = projected * projected
    lanes = width // 2
    column = jnp.sum((squares[:, :lanes] + squares[:, lanes:]).T, axis=0, keepdims=True)
    stats[tp] = jnp.broadcast_to(column, stats.shape[1:])
    for k in range(1, n_tp):
        start(stats.at[tp], stats.at[tp], s_send.at[k], s_recv.at[k], sp, lax.rem(tp + k, n_tp))
    for k in range(1, n_tp):
        recv(stats.at[lax.rem(tp + n_tp - k, n_tp)], s_send.at[k], s_recv.at[k])
    summed = functools.reduce(jnp.add, [stats[t, 0:1, :] for t in range(n_tp)])
    norm = lax.rsqrt(summed * (1.0 / D) + EPSILON)
    norm = jnp.broadcast_to(norm, (lanes, ROWS)).T
    for k in (0, 1):
        cols = slice(k * lanes, (k + 1) * lanes)
        mixed_ref[:, cols] = (projected[:, cols] * norm * gain_ref[:, cols]).astype(jnp.bfloat16)

    @pl.when(sp < BLOCKS - 1)
    def _():
        sent(driven.at[pl.ds(8, 8)], halo_send, halo_recv)

    ring_sent(token_part, *tok_sems, ROWS)
    for h in range(LOCAL):
        @pl.when(leaves(h))
        def _(h=h):
            sent(q_ref.at[h], qz_send.at[h], qz_recv.at[h])
            sent(kv_ref.at[h], kz_send.at[h], kz_recv.at[h])
    for j in range(LOCAL):
        block = all_ref.at[0]
        part = all_ref.at[0, pl.ds(0, half)]
        for k in (0, 1):
            sent(block, x_send.at[j, k], x_recv.at[j, k])
            sent(part, x_send.at[j, 2 + k], x_recv.at[j, 2 + k])
            sent(part, d_send.at[j, 3 + k], d_recv.at[j, 3 + k])
        for k in (0, 1, 2):
            sent(block, d_send.at[j, k], d_recv.at[j, k])

        @pl.when(jnp.logical_not(stays(j)))
        def _(j=j):
            sent(results.at[j], rz_send.at[j], rz_recv.at[j])
            sent(logs.at[j], lz_send.at[j], lz_recv.at[j])

        @pl.when(jnp.logical_not(here(j)))
        def _(j=j):
            recv(logs_ref.at[j], lz_send.at[j], lz_recv.at[j])

        ring_sent(*head_ring(j))
    ring_sent(conv_part, *conv_sems, wc_rows)
    for k in range(1, n_tp):
        sent(rows_of(wcol, 0, wa_rows), wa_send.at[k], wa_recv.at[k])
        sent(rows_of(wconv, 0, wc_rows), wc_send.at[k], wc_recv.at[k])
        sent(stats.at[0], s_send.at[k], s_recv.at[k])


def layer(tokens, small, matrices):
    dma = pltpu.SemaphoreType.DMA
    wa, wc = matrices[-2:]
    wqup, wkvup = matrices[5:7]
    wa_rows, wc_rows = wa.shape[0], wc.shape[0]
    n_tp = 2 * NY
    width = wa.shape[1] // n_tp
    bf16, f32 = jnp.bfloat16, jnp.float32
    total = sum(m.shape[1] for m in matrices[:5]) + 128
    sems = [dma((7,)), dma, dma]
    for shape in ((4,), (5,), (4,), (4,), (4, 4), (4, 5), (8,), (8,), (4,), (5,), (4,), (4,), (4, 4), (4, 5), (8,)):
        sems += [dma(shape), dma(shape)]
    return pl.pallas_call(
        layer_kernel,
        out_shape=(
            jax.ShapeDtypeStruct((ROWS, width), bf16),
            jax.ShapeDtypeStruct((LOCAL, 8, ROWS), f32),
        ),
        in_specs=[pl.BlockSpec(memory_space=VMEM)] * (1 + len(small))
        + [pl.BlockSpec(memory_space=pl.ANY)] * len(matrices),
        out_specs=(pl.BlockSpec(memory_space=VMEM),) * 2,
        scratch_shapes=[
            pltpu.VMEM((ROWS, D), bf16),
            pltpu.VMEM((D, total), bf16),
            pltpu.VMEM(wqup.shape, bf16),
            pltpu.VMEM(wkvup.shape, bf16),
            pltpu.VMEM((ROWS, total), f32),
            pltpu.VMEM((ROWS, 128), f32),
            pltpu.VMEM((ROWS + 16, wc_rows), bf16),
            pltpu.VMEM((LOCAL, KVR, ROWS), bf16),
            pltpu.VMEM((LOCAL, QK, ROWS), bf16),
            pltpu.VMEM((wc_rows, ROWS), bf16),
            pltpu.VMEM((BLOCKS, KVR, ROWS), bf16),
            pltpu.VMEM((QK, LOCAL * ROWS), bf16),
            pltpu.VMEM((wa_rows * n_tp, width), bf16),
            pltpu.VMEM((wc_rows * n_tp, width), bf16),
            pltpu.VMEM((wc_rows * n_tp, ROWS), bf16),
            pltpu.VMEM((wa_rows * n_tp, ROWS), bf16),
            pltpu.VMEM((LOCAL, VDIM, ROWS), bf16),
            pltpu.VMEM((LOCAL, 8, ROWS), f32),
            pltpu.VMEM((n_tp, 8, ROWS), f32),
            pltpu.VMEM((1, LOCAL * ROWS), f32),
            pltpu.VMEM((1, LOCAL * ROWS), f32),
            pltpu.VMEM((VDIM, LOCAL * ROWS), f32),
        ] + sems,
        compiler_params=pltpu.CompilerParams(
            collective_id=1, has_side_effects=True, vmem_limit_bytes=60 * 2**20,
        ),
        name="layer_rest",
    )(tokens, *small, *matrices)


def rotation(positions, width):
    freqs = THETA ** (-jnp.arange(0, width, 2, dtype=jnp.float32) / width)
    angles = freqs[:, None] * positions.astype(jnp.float32)[None, :]
    return (jnp.cos(angles), jnp.sin(angles))


def body(
    tokens,
    pre_gain,
    outer_gate_weight,
    inner_gate_weight,
    source_weight,
    conv_taps,
    q_down_weight,
    q_norm_gain,
    q_up_weight,
    kv_down_weight,
    rope_key_weight,
    kv_norm_gain,
    kv_up_weight,
    attn_out_weight,
    conv_out_weight,
    post_gain,
):
    token_rows = tokens.shape[0]
    query_pos = lax.axis_index("sp") * token_rows + jnp.arange(token_rows, dtype=jnp.int32)
    cosine, sine = rotation(query_pos, ROPE)
    small = (
        pre_gain[None, :], conv_taps, q_norm_gain[None, :], kv_norm_gain[None, :], post_gain[None, :],
        rope_key_weight.T, cosine, sine,
    )
    matrices = (
        outer_gate_weight, inner_gate_weight, source_weight, q_down_weight, kv_down_weight,
        q_up_weight, kv_up_weight, attn_out_weight, conv_out_weight,
    )
    mixed, logs = layer(tokens, small, matrices)
    return (mixed, logs[:, 0, :])


def solution(mesh):
    placed = (
        P("sp", "tp"),
        P(),
        P(None, "tp"),
        P(None, "tp"),
        P(None, "tp"),
        P(None, "tp"),
        P(),
        P(),
        P(None, "tp"),
        P(),
        P(),
        P(),
        P(None, "tp"),
        P("tp", None),
        P("tp", None),
        P("tp"),
    )
    return jax.shard_map(
        body, mesh=mesh, in_specs=placed, out_specs=(P("sp", "tp"), P("tp", "sp")), check_vma=False
    )
```

```python
import functools
import math

import jax
import jax.numpy as jnp
from jax import lax
from jax.experimental import pallas as pl
from jax.experimental.pallas import tpu as pltpu
from jax.sharding import PartitionSpec as P

D = 2048
NOPE = 64
ROPE = 32
VDIM = 64
TAPS = 3
NZ, NX, NY = 8, 4, 4
ROWS = 384
KVR = NOPE + ROPE + VDIM
QK = NOPE + ROPE
LOCAL = 4
BLOCKS = NZ * NX

EPSILON = 1e-06
THETA = 500000.0
NEGATIVE = -1e30
LOG2E = math.log2(math.e)
MESH = pl.DeviceIdType.MESH
VMEM = pltpu.MemorySpace.VMEM


def side(z):
    return lax.rem(lax.div(z + 1, 2), 2)


def plane(j, core):
    return 2 * j + lax.rem(j + core, 2)


def remote(src, dst, send, recv, sp, tp):
    return pltpu.make_async_remote_copy(
        src_ref=src, dst_ref=dst, send_sem=send, recv_sem=recv,
        device_id=(sp, tp), device_id_type=MESH,
    )


def attention_step(kv_ref, q_ref, m_ref, l_ref, acc_ref, block, group, active, offset):
    scale = QK ** -0.5 * LOG2E
    width = active * ROWS
    cols = slice(0, width)
    scores = []
    for g in range(group):
        keys = kv_ref[block + g, 0:QK, :].T
        value = jnp.dot(keys, q_ref[:, cols], preferred_element_type=jnp.float32)
        if offset is not None:
            start = width - ROWS
            key = lax.broadcasted_iota(jnp.int32, value.shape, 0) + (offset + g * ROWS)
            row = lax.broadcasted_iota(jnp.int32, value.shape, 1) - start
            keep = key <= row
            if start:
                keep = jnp.logical_or(keep, row < 0)
            value = jnp.where(keep, value, NEGATIVE)
        scores.append(value)
    old = m_ref[:, cols]
    top = functools.reduce(jnp.maximum, [jnp.max(v, axis=0, keepdims=True) for v in scores])
    fresh = jnp.maximum(old, top * scale)
    shrink = jnp.exp2(old - fresh)
    weights = [jnp.exp2(v * scale - fresh) for v in scores]
    m_ref[:, cols] = fresh
    l_ref[:, cols] = l_ref[:, cols] * shrink + sum(
        jnp.sum(w, axis=0, keepdims=True) for w in weights
    )
    acc_ref[:, cols] = acc_ref[:, cols] * shrink + sum(
        jnp.dot(kv_ref[block + g, QK:KVR, :], w.astype(jnp.bfloat16), preferred_element_type=jnp.float32)
        for g, w in enumerate(weights)
    )


AHEAD_A, AHEAD_B = 4, 2

GROUPS = {4: 1, 3: 1, 2: 2, 1: 4}


def attend_plane(kv_ref, q_ref, state, p, core, x):
    direct = side(p) == core
    pair = lax.div(p, 2)
    later = LOCAL - pair - lax.rem(p, 2)
    for active in range(1, LOCAL + 1):
        group = GROUPS[active]

        @pl.when(jnp.logical_and(direct, pair == LOCAL - active))
        def _(active=active, group=group):
            def advance(i, carry):
                attention_step(kv_ref, q_ref, *state, p * NX + i * group, group, active,
                               (i * group - x) * ROWS)
                return carry

            lax.fori_loop(0, NX // group, advance, 0)

        @pl.when(jnp.logical_and(jnp.logical_not(direct), later == active))
        def _(active=active, group=group):
            def advance(i, carry):
                attention_step(kv_ref, q_ref, *state, p * NX + i * group, group, active, None)
                return carry

            lax.fori_loop(0, NX // group, advance, 0)


def layer_kernel(
    tokens_ref, pre_ref, taps_ref, qgain_ref, kvgain_ref, gain_ref, rope_ref, cos_ref, sin_ref,
    wo_ref, wi_ref, ws_ref, wq_ref, wkv_ref, wqup_ref, wkvup_ref, wa_ref, wc_ref,
    mixed_ref, logs_ref,
    tok, wall, wqup, wkvup, sums, squares, driven, kv_ref, q_ref, conv_ref,
    all_ref, mine_ref, wcol, wconv, convs, heads, results, logs, stats, m_ref, l_ref, acc_ref,
    load_sem, halo_send, halo_recv, ty_send, ty_recv, td_send, td_recv,
    kz_send, kz_recv, qz_send, qz_recv, x_send, x_recv, d_send, d_recv,
    wa_send, wa_recv, wc_send, wc_recv, cy_send, cy_recv, cd_send, cd_recv,
    rz_send, rz_recv, lz_send, lz_recv, hy_send, hy_recv, hd_send, hd_recv, s_send, s_recv,
):
    sp = lax.axis_index("sp")
    tp = lax.axis_index("tp")
    z, x = lax.div(sp, NX), lax.rem(sp, NX)
    core, y = lax.rem(tp, 2), lax.div(tp, 2)
    other = 1 - core
    mate = tp + 1 - 2 * core
    xp, xm, xf = (lax.rem(x + k, NX) for k in (1, NX - 1, 2))
    up, down, far = (lax.rem(y + k, NY) * 2 + core for k in (1, NY - 1, 2))
    flip = other - core
    to_core = side(z)
    owner = lax.div(z, LOCAL)
    half = KVR // 2
    n_tp = 2 * NY

    peers = [(lax.rem(z + k, NZ) * NX + x, 2 * y + c) for k in range(1, NZ) for c in (0, 1)]
    peers += [(z * NX + xp, tp), (z * NX + xm, tp)]
    peers += [(lax.rem(sp + k, BLOCKS), tp) for k in (1, BLOCKS - 1)]
    peers += [(sp, lax.rem(tp + k, n_tp)) for k in range(1, n_tp)]

    edges = [0]
    for ref in (wkv_ref, wq_ref, wo_ref, wi_ref, ws_ref):
        edges.append(edges[-1] + ref.shape[1])
    loads = [
        pltpu.make_async_copy(ref, wall.at[:, pl.ds(edges[i], ref.shape[1])], load_sem.at[i])
        for i, ref in enumerate((wkv_ref, wq_ref, wo_ref, wi_ref, ws_ref))
    ]
    loads += [
        pltpu.make_async_copy(wkvup_ref, wkvup, load_sem.at[5]),
        pltpu.make_async_copy(wqup_ref, wqup, load_sem.at[6]),
    ]
    for c in loads:
        c.start()
    barrier = pltpu.get_barrier_semaphore()
    for peer in peers:
        pl.semaphore_signal(barrier, inc=1, device_id=peer, device_id_type=MESH)
    pad = jnp.zeros((128 - ROPE, rope_ref.shape[1]), jnp.float32)
    wall[:, pl.ds(edges[-1], 128)] = (
        jnp.concatenate([rope_ref[...].astype(jnp.float32), pad], axis=0).T.astype(jnp.bfloat16)
    )
    pl.semaphore_wait(barrier, len(peers))

    keep = jnp.logical_and(owner == core, to_core == core)
    own_head = z - LOCAL * core
    my_pair = lax.div(z, 2)

    def slot(ref, j):
        return ref.at[:, pl.ds(pl.multiple_of((LOCAL - 1 - j) * ROWS, ROWS), ROWS)]

    def start(src, dst, s, r, to_sp, to_tp):
        remote(src, dst, s, r, to_sp, to_tp).start()

    def recv(dst, s, r):
        remote(dst, dst, s, r, sp, mate).wait_recv()

    def sent(src, s, r):
        remote(src, src, s, r, sp, mate).wait_send()

    def leaves(h):
        return jnp.logical_not(jnp.logical_and(keep, own_head == h))

    def ring_start(source, part, y_s, y_r, d_s, d_r, rows):
        start(source, part(tp, 0, rows), y_s(0), y_r(0), sp, up)
        start(source, part(tp, 0, rows), y_s(1), y_r(1), sp, down)
        start(source, part(tp, 0, rows), d_s(0), d_r(0), sp, mate)

    def ring_middle(part, y_s, y_r, d_s, d_r, rows):
        cut = rows // 2
        recv(part(down, 0, rows), y_s(0), y_r(0))
        start(part(down, 0, cut), part(down, 0, cut), y_s(2), y_r(2), sp, up)
        start(part(down, 0, rows), part(down, 0, rows), d_s(1), d_r(1), sp, mate)
        recv(part(up, 0, rows), y_s(1), y_r(1))
        start(part(up, cut, cut), part(up, cut, cut), y_s(3), y_r(3), sp, down)
        start(part(up, 0, rows), part(up, 0, rows), d_s(2), d_r(2), sp, mate)

    def ring_end(part, y_s, y_r, d_s, d_r, rows):
        cut = rows // 2
        for k in (0, 1):
            recv(part(far, k * cut, cut), y_s(2 + k), y_r(2 + k))
            start(part(far, k * cut, cut), part(far, k * cut, cut), d_s(3 + k), d_r(3 + k), sp, mate)

    def ring_far(part, d_s, d_r, rows):
        cut = rows // 2
        for k in (0, 1):
            recv(part(far + flip, k * cut, cut), d_s(3 + k), d_r(3 + k))

    def ring_recv(part, d_s, d_r, rows):
        recv(part(mate, 0, rows), d_s(0), d_r(0))
        recv(part(down + flip, 0, rows), d_s(1), d_r(1))
        recv(part(up + flip, 0, rows), d_s(2), d_r(2))
        ring_far(part, d_s, d_r, rows)

    def ring_sent(part, y_s, y_r, d_s, d_r, rows):
        cut = rows // 2
        for k in (0, 1):
            sent(part(tp, 0, rows), y_s(k), y_r(k))
            sent(part(tp, 0, cut), y_s(2 + k), y_r(2 + k))
            sent(part(tp, 0, cut), d_s(3 + k), d_r(3 + k))
        for k in (0, 1, 2):
            sent(part(tp, 0, rows), d_s(k), d_r(k))

    part_width = tokens_ref.shape[1]

    def token_part(owner_tp, first=0, count=ROWS):
        return tok.at[pl.ds(first, count), pl.ds(pl.multiple_of(owner_tp * part_width, part_width), part_width)]

    tok_sems = [lambda k, ref=ref: ref.at[k] for ref in (ty_send, ty_recv, td_send, td_recv)]
    ring_start(tokens_ref, token_part, *tok_sems, ROWS)
    tok[:, pl.ds(pl.multiple_of(tp * part_width, part_width), part_width)] = tokens_ref[...]

    def project(chip, fresh):
        share = 2 * part_width
        cols = pl.ds(pl.multiple_of(chip * share, share), share)
        wide = tok[:, cols].astype(jnp.float32)
        part = wide * wide
        part = functools.reduce(jnp.add, [part[:, k : k + 128] for k in range(0, share, 128)])
        value = jnp.dot((wide * pre_ref[:, cols]).astype(jnp.bfloat16), wall[cols, :],
                        preferred_element_type=jnp.float32)
        squares[...] = part if fresh else squares[...] + part
        sums[...] = value if fresh else sums[...] + value

    recv(token_part(mate), td_send.at[0], td_recv.at[0])
    for c in loads[:5]:
        c.wait()
    project(y, True)
    ring_middle(token_part, *tok_sems, ROWS)
    recv(token_part(down + flip), td_send.at[1], td_recv.at[1])
    project(lax.div(down, 2), False)
    ring_end(token_part, *tok_sems, ROWS)
    recv(token_part(up + flip), td_send.at[2], td_recv.at[2])
    project(lax.div(up, 2), False)
    ring_far(token_part, tok_sems[2], tok_sems[3], ROWS)
    def rows_of(ref, index, count, first=0):
        return ref.at[pl.ds(pl.multiple_of(index, count) + first, count)]

    wa_rows, wc_rows = LOCAL * VDIM, convs.shape[0] // n_tp
    width = wcol.shape[1]

    def columns(ref, owner_tp):
        return ref.at[:, pl.ds(pl.multiple_of(owner_tp * width, width), width)]

    def conv_part(owner_tp, first=0, count=wc_rows):
        return convs.at[pl.ds(pl.multiple_of(owner_tp * wc_rows + first, 16), count)]

    for k in range(1, n_tp):
        to = lax.rem(tp + k, n_tp)
        start(columns(wa_ref, to), rows_of(wcol, tp * wa_rows, wa_rows), wa_send.at[k], wa_recv.at[k], sp, to)
        start(columns(wc_ref, to), rows_of(wconv, tp * wc_rows, wc_rows), wc_send.at[k], wc_recv.at[k], sp, to)
    own_wa = pltpu.make_async_copy(columns(wa_ref, tp), rows_of(wcol, tp * wa_rows, wa_rows), wa_send.at[0])
    own_wc = pltpu.make_async_copy(columns(wc_ref, tp), rows_of(wconv, tp * wc_rows, wc_rows), wc_send.at[0])
    own_wa.start()
    own_wc.start()
    project(lax.div(far, 2), False)
    factor = lax.rsqrt(jnp.sum(squares[...], axis=1, keepdims=True) * (1.0 / D) + EPSILON)

    def normed(first, last, gain):
        value = sums[:, first:last] * factor
        mean = jnp.sum(value * value, axis=1, keepdims=True) * (1.0 / (last - first))
        return (value * lax.rsqrt(mean + EPSILON) * gain).astype(jnp.bfloat16)

    cosine, sine = cos_ref[...], sin_ref[...]

    def rotate(first, second):
        return jnp.concatenate(
            [first * cosine - second * sine, second * cosine + first * sine], axis=0
        ).astype(jnp.bfloat16)

    def plane_at(i):
        step = lax.div(i + 1, 2)
        return lax.rem(z + jnp.where(lax.rem(i, 2) == 1, step, NZ - step), NZ)

    def to_planes(send):
        for i in range(NZ):
            target = plane_at(jnp.int32(i))

            @pl.when(jnp.logical_and(lax.div(target, LOCAL) == core, leaves(target - LOCAL * core)))
            def _(target=target):
                send(target - LOCAL * core, target * NX + x, 2 * y + to_core)

    def send_keys(h, to_sp, to_tp):
        start(kv_ref.at[h], all_ref.at[sp], kz_send.at[h], kz_recv.at[my_pair], to_sp, to_tp)

    def send_queries(h, to_sp, to_tp):
        start(q_ref.at[h], slot(mine_ref, my_pair), qz_send.at[h], qz_recv.at[my_pair], to_sp, to_tp)

    loads[6].wait()
    query = jnp.dot(normed(edges[1], edges[2], qgain_ref[...]), wqup[...], preferred_element_type=jnp.float32).T
    for h in range(LOCAL):
        first = h * QK
        q_ref[h, 0:NOPE] = query[first : first + NOPE].astype(jnp.bfloat16)
        q_ref[h, NOPE:QK] = rotate(query[first + NOPE : first + NOPE + ROPE // 2],
                                   query[first + NOPE + ROPE // 2 : first + QK])
    to_planes(send_queries)

    loads[5].wait()
    keyvals = jnp.dot(normed(edges[0], edges[1], kvgain_ref[...]), wkvup[...], preferred_element_type=jnp.float32).T
    turn = (sums[:, edges[-1] : edges[-1] + 128] * factor).T
    rope_key = rotate(turn[: ROPE // 2], turn[ROPE // 2 : ROPE])
    for h in range(LOCAL):
        first = h * (NOPE + VDIM)
        kv_ref[h, 0:NOPE] = keyvals[first : first + NOPE].astype(jnp.bfloat16)
        kv_ref[h, NOPE:QK] = rope_key
        kv_ref[h, QK:KVR] = keyvals[first + NOPE : first + NOPE + VDIM].astype(jnp.bfloat16)
    to_planes(send_keys)
    for h in range(LOCAL):
        @pl.when(jnp.logical_not(leaves(h)))
        def _(h=h):
            all_ref[sp] = kv_ref[h]
            mine_ref[:, pl.ds(pl.multiple_of((LOCAL - 1 - my_pair) * ROWS, ROWS), ROWS)] = q_ref[h]

    outer, inner, source = (
        (sums[:, edges[k] : edges[k + 1]] * factor).astype(jnp.bfloat16) for k in (2, 3, 4)
    )
    driven[pl.ds(16, ROWS), :] = (inner.astype(jnp.float32) * source.astype(jnp.float32)).astype(jnp.bfloat16)

    @pl.when(sp < BLOCKS - 1)
    def _():
        start(driven.at[pl.ds(ROWS + 8, 8)], driven.at[pl.ds(8, 8)], halo_send, halo_recv, sp + 1, tp)

    @pl.when(sp == 0)
    def _():
        driven[pl.ds(8, 8), :] = jnp.zeros((8, driven.shape[1]), jnp.bfloat16)

    @pl.when(sp > 0)
    def _():
        recv(driven.at[pl.ds(8, 8)], halo_send, halo_recv)

    extended = driven[pl.ds(8, ROWS + 8), :].astype(jnp.float32)
    taps = taps_ref[...].astype(jnp.float32)
    convolved = functools.reduce(
        jnp.add,
        [taps[k : k + 1] * extended[9 - TAPS + k : 9 - TAPS + k + ROWS] for k in range(TAPS)],
    )
    conv_ref[...] = (outer.astype(jnp.float32) * convolved).T.astype(jnp.bfloat16)

    conv_sems = [lambda k, ref=ref: ref.at[k] for ref in (cy_send, cy_recv, cd_send, cd_recv)]
    ring_start(conv_ref, conv_part, *conv_sems, wc_rows)
    convs[pl.ds(pl.multiple_of(tp * wc_rows, wc_rows), wc_rows), :] = conv_ref[...]

    m_ref[...] = jnp.full_like(m_ref, NEGATIVE)
    l_ref[...] = jnp.zeros_like(l_ref)
    acc_ref[...] = jnp.zeros_like(acc_ref)

    def z_wait(j, dst, s, r):
        @pl.when(jnp.logical_not(jnp.logical_and(keep, plane(j, core) == z)))
        def _():
            recv(dst, s, r)

    def stage_a(p):
        @pl.when(side(p) == core)
        def _():
            j = lax.div(p, 2)
            block = all_ref.at[p * NX + x]
            z_wait(j, block, kz_send.at[0], kz_recv.at[j])
            start(block, block, x_send.at[j, 0], x_recv.at[j, 0], z * NX + xp, tp)
            start(block, block, x_send.at[j, 1], x_recv.at[j, 1], z * NX + xm, tp)
            start(block, block, d_send.at[j, 0], d_recv.at[j, 0], sp, mate)

    def stage_b(p):
        @pl.when(side(p) == core)
        def _():
            j = lax.div(p, 2)
            low, high = all_ref.at[p * NX + xm], all_ref.at[p * NX + xp]
            recv(low, x_send.at[j, 0], x_recv.at[j, 0])
            part = all_ref.at[p * NX + xm, pl.ds(0, half)]
            start(part, part, x_send.at[j, 2], x_recv.at[j, 2], z * NX + xp, tp)
            start(low, low, d_send.at[j, 1], d_recv.at[j, 1], sp, mate)
            recv(high, x_send.at[j, 1], x_recv.at[j, 1])
            part = all_ref.at[p * NX + xp, pl.ds(half, half)]
            start(part, part, x_send.at[j, 3], x_recv.at[j, 3], z * NX + xm, tp)
            start(high, high, d_send.at[j, 2], d_recv.at[j, 2], sp, mate)

    def stage_c(p):
        j = lax.div(p, 2)
        parts = [all_ref.at[p * NX + xf, pl.ds(k * half, half)] for k in (0, 1)]

        @pl.when(side(p) == core)
        def _():
            for k in (0, 1):
                recv(parts[k], x_send.at[j, 2 + k], x_recv.at[j, 2 + k])
                start(parts[k], parts[k], d_send.at[j, 3 + k], d_recv.at[j, 3 + k], sp, mate)

        @pl.when(side(p) != core)
        def _():
            for k, column in enumerate((x, xm, xp)):
                recv(all_ref.at[p * NX + column], d_send.at[j, k], d_recv.at[j, k])
            for k in (0, 1):
                recv(parts[k], d_send.at[j, 3 + k], d_recv.at[j, 3 + k])

    for i in range(AHEAD_A):
        stage_a(plane_at(jnp.int32(i)))
        if 0 <= i + AHEAD_B - AHEAD_A:
            stage_b(plane_at(jnp.int32(i + AHEAD_B - AHEAD_A)))
    for j in range(LOCAL):
        z_wait(j, slot(mine_ref, j), qz_send.at[0], qz_recv.at[j])

    def work(i, carry):
        @pl.when(i + AHEAD_A < NZ)
        def _():
            stage_a(plane_at(i + AHEAD_A))

        @pl.when(i + AHEAD_B < NZ)
        def _():
            stage_b(plane_at(i + AHEAD_B))

        @pl.when(i == NZ - 2)
        def _():
            ring_middle(conv_part, *conv_sems, wc_rows)

        p = plane_at(i)
        stage_c(p)
        attend_plane(all_ref, mine_ref, (m_ref, l_ref, acc_ref), p, core, x)
        return carry

    lax.fori_loop(0, NZ, work, 0)
    ring_end(conv_part, *conv_sems, wc_rows)

    total = m_ref[...] * (1.0 / LOG2E) + jnp.log(l_ref[...])
    scaled = acc_ref[...] * (1.0 / l_ref[...])
    to = 2 * y + owner

    def head_rows(owner_tp, h, first=0, count=VDIM):
        return heads.at[pl.ds(pl.multiple_of((owner_tp * LOCAL + h) * VDIM + first, 16), count)]

    head = lax.rem(z, LOCAL)
    for j in range(LOCAL):
        cols = slice((LOCAL - 1 - j) * ROWS, (LOCAL - j) * ROWS)
        results[j] = scaled[:, cols].astype(jnp.bfloat16)
        logs[j] = jnp.broadcast_to(total[:, cols], logs.shape[1:])

    def stays(j):
        return jnp.logical_and(keep, plane(j, core) == z)

    for j in range(LOCAL):
        @pl.when(jnp.logical_not(stays(j)))
        def _(j=j):
            start(results.at[j], head_rows(to, head), rz_send.at[j], rz_recv.at[head], plane(j, core) * NX + x, to)
            start(logs.at[j], logs_ref.at[head], lz_send.at[j], lz_recv.at[head], plane(j, core) * NX + x, to)
    for j in range(LOCAL):
        @pl.when(stays(j))
        def _(j=j):
            heads[pl.ds(pl.multiple_of((to * LOCAL + head) * VDIM, VDIM), VDIM), :] = results[j]
            logs_ref[head] = logs[j]

    ring_recv(conv_part, conv_sems[2], conv_sems[3], wc_rows)
    own_wc.wait()
    own_wa.wait()
    for k in range(1, n_tp):
        source = lax.rem(tp + n_tp - k, n_tp)
        recv(rows_of(wconv, source * wc_rows, wc_rows), wc_send.at[k], wc_recv.at[k])
        recv(rows_of(wcol, source * wa_rows, wa_rows), wa_send.at[k], wa_recv.at[k])
    turned = (((0,), (0,)), ((), ()))
    projected = lax.dot_general(convs[...], wconv[...], turned, preferred_element_type=jnp.float32)

    def here(h):
        return jnp.logical_and(keep, LOCAL * core + h == z)

    def head_ring(h):
        return (
            lambda owner_tp, first, count: head_rows(owner_tp, h, first, count),
            *[lambda k, ref=ref: ref.at[h, k] for ref in (hy_send, hy_recv, hd_send, hd_recv)],
            VDIM,
        )

    for step in range(LOCAL + 2):
        if step < LOCAL:
            h = step
            mine = head_rows(tp, h)

            @pl.when(jnp.logical_not(here(h)))
            def _(h=h, mine=mine):
                recv(mine, rz_send.at[h], rz_recv.at[h])

            start(mine, mine, hy_send.at[h, 0], hy_recv.at[h, 0], sp, up)
            start(mine, mine, hy_send.at[h, 1], hy_recv.at[h, 1], sp, down)
            start(mine, mine, hd_send.at[h, 0], hd_recv.at[h, 0], sp, mate)
        if 1 <= step <= LOCAL:
            ring_middle(*head_ring(step - 1))
        if step >= 2:
            ring_end(*head_ring(step - 2))
    for h in range(LOCAL):
        part, _, _, d_s, d_r, rows = head_ring(h)
        ring_recv(part, d_s, d_r, rows)
    projected = projected + lax.dot_general(heads[...], wcol[...], turned, preferred_element_type=jnp.float32)

    squares = projected * projected
    lanes = width // 2
    column = jnp.sum((squares[:, :lanes] + squares[:, lanes:]).T, axis=0, keepdims=True)
    stats[tp] = jnp.broadcast_to(column, stats.shape[1:])
    for k in range(1, n_tp):
        start(stats.at[tp], stats.at[tp], s_send.at[k], s_recv.at[k], sp, lax.rem(tp + k, n_tp))
    for k in range(1, n_tp):
        recv(stats.at[lax.rem(tp + n_tp - k, n_tp)], s_send.at[k], s_recv.at[k])
    summed = functools.reduce(jnp.add, [stats[t, 0:1, :] for t in range(n_tp)])
    norm = lax.rsqrt(summed * (1.0 / D) + EPSILON)
    norm = jnp.broadcast_to(norm, (lanes, ROWS)).T
    for k in (0, 1):
        cols = slice(k * lanes, (k + 1) * lanes)
        mixed_ref[:, cols] = (projected[:, cols] * norm * gain_ref[:, cols]).astype(jnp.bfloat16)

    @pl.when(sp < BLOCKS - 1)
    def _():
        sent(driven.at[pl.ds(8, 8)], halo_send, halo_recv)

    ring_sent(token_part, *tok_sems, ROWS)
    for h in range(LOCAL):
        @pl.when(leaves(h))
        def _(h=h):
            sent(q_ref.at[h], qz_send.at[h], qz_recv.at[h])
            sent(kv_ref.at[h], kz_send.at[h], kz_recv.at[h])
    for j in range(LOCAL):
        block = all_ref.at[0]
        part = all_ref.at[0, pl.ds(0, half)]
        for k in (0, 1):
            sent(block, x_send.at[j, k], x_recv.at[j, k])
            sent(part, x_send.at[j, 2 + k], x_recv.at[j, 2 + k])
            sent(part, d_send.at[j, 3 + k], d_recv.at[j, 3 + k])
        for k in (0, 1, 2):
            sent(block, d_send.at[j, k], d_recv.at[j, k])

        @pl.when(jnp.logical_not(stays(j)))
        def _(j=j):
            sent(results.at[j], rz_send.at[j], rz_recv.at[j])
            sent(logs.at[j], lz_send.at[j], lz_recv.at[j])

        @pl.when(jnp.logical_not(here(j)))
        def _(j=j):
            recv(logs_ref.at[j], lz_send.at[j], lz_recv.at[j])

        ring_sent(*head_ring(j))
    ring_sent(conv_part, *conv_sems, wc_rows)
    for k in range(1, n_tp):
        sent(rows_of(wcol, 0, wa_rows), wa_send.at[k], wa_recv.at[k])
        sent(rows_of(wconv, 0, wc_rows), wc_send.at[k], wc_recv.at[k])
        sent(stats.at[0], s_send.at[k], s_recv.at[k])


def layer(tokens, small, matrices):
    dma = pltpu.SemaphoreType.DMA
    wa, wc = matrices[-2:]
    wqup, wkvup = matrices[5:7]
    wa_rows, wc_rows = wa.shape[0], wc.shape[0]
    n_tp = 2 * NY
    width = wa.shape[1] // n_tp
    bf16, f32 = jnp.bfloat16, jnp.float32
    total = sum(m.shape[1] for m in matrices[:5]) + 128
    sems = [dma((7,)), dma, dma]
    for shape in ((4,), (5,), (4,), (4,), (4, 4), (4, 5), (8,), (8,), (4,), (5,), (4,), (4,), (4, 4), (4, 5), (8,)):
        sems += [dma(shape), dma(shape)]
    return pl.pallas_call(
        layer_kernel,
        out_shape=(
            jax.ShapeDtypeStruct((ROWS, width), bf16),
            jax.ShapeDtypeStruct((LOCAL, 8, ROWS), f32),
        ),
        in_specs=[pl.BlockSpec(memory_space=VMEM)] * (1 + len(small))
        + [pl.BlockSpec(memory_space=pl.ANY)] * len(matrices),
        out_specs=(pl.BlockSpec(memory_space=VMEM),) * 2,
        scratch_shapes=[
            pltpu.VMEM((ROWS, D), bf16),
            pltpu.VMEM((D, total), bf16),
            pltpu.VMEM(wqup.shape, bf16),
            pltpu.VMEM(wkvup.shape, bf16),
            pltpu.VMEM((ROWS, total), f32),
            pltpu.VMEM((ROWS, 128), f32),
            pltpu.VMEM((ROWS + 16, wc_rows), bf16),
            pltpu.VMEM((LOCAL, KVR, ROWS), bf16),
            pltpu.VMEM((LOCAL, QK, ROWS), bf16),
            pltpu.VMEM((wc_rows, ROWS), bf16),
            pltpu.VMEM((BLOCKS, KVR, ROWS), bf16),
            pltpu.VMEM((QK, LOCAL * ROWS), bf16),
            pltpu.VMEM((wa_rows * n_tp, width), bf16),
            pltpu.VMEM((wc_rows * n_tp, width), bf16),
            pltpu.VMEM((wc_rows * n_tp, ROWS), bf16),
            pltpu.VMEM((wa_rows * n_tp, ROWS), bf16),
            pltpu.VMEM((LOCAL, VDIM, ROWS), bf16),
            pltpu.VMEM((LOCAL, 8, ROWS), f32),
            pltpu.VMEM((n_tp, 8, ROWS), f32),
            pltpu.VMEM((1, LOCAL * ROWS), f32),
            pltpu.VMEM((1, LOCAL * ROWS), f32),
            pltpu.VMEM((VDIM, LOCAL * ROWS), f32),
        ] + sems,
        compiler_params=pltpu.CompilerParams(
            collective_id=1, has_side_effects=True, vmem_limit_bytes=60 * 2**20,
        ),
        name="layer_rest",
    )(tokens, *small, *matrices)


def rotation(positions, width):
    freqs = THETA ** (-jnp.arange(0, width, 2, dtype=jnp.float32) / width)
    angles = freqs[:, None] * positions.astype(jnp.float32)[None, :]
    return (jnp.cos(angles), jnp.sin(angles))


def body(
    tokens,
    pre_gain,
    outer_gate_weight,
    inner_gate_weight,
    source_weight,
    conv_taps,
    q_down_weight,
    q_norm_gain,
    q_up_weight,
    kv_down_weight,
    rope_key_weight,
    kv_norm_gain,
    kv_up_weight,
    attn_out_weight,
    conv_out_weight,
    post_gain,
):
    token_rows = tokens.shape[0]
    query_pos = lax.axis_index("sp") * token_rows + jnp.arange(token_rows, dtype=jnp.int32)
    cosine, sine = rotation(query_pos, ROPE)
    small = (
        pre_gain[None, :], conv_taps, q_norm_gain[None, :], kv_norm_gain[None, :], post_gain[None, :],
        rope_key_weight.T, cosine, sine,
    )
    matrices = (
        outer_gate_weight, inner_gate_weight, source_weight, q_down_weight, kv_down_weight,
        q_up_weight, kv_up_weight, attn_out_weight, conv_out_weight,
    )
    mixed, logs = layer(tokens, small, matrices)
    return (mixed, logs[:, 0, :])


def solution(mesh):
    placed = (
        P("sp", "tp"),
        P(),
        P(None, "tp"),
        P(None, "tp"),
        P(None, "tp"),
        P(None, "tp"),
        P(),
        P(),
        P(None, "tp"),
        P(),
        P(),
        P(),
        P(None, "tp"),
        P("tp", None),
        P("tp", None),
        P("tp"),
    )
    return jax.shard_map(
        body, mesh=mesh, in_specs=placed, out_specs=(P("sp", "tp"), P("tp", "sp")), check_vma=False
    )
```

```python
import functools
import math

import jax
import jax.numpy as jnp
from jax import lax
from jax.experimental import pallas as pl
from jax.experimental.pallas import tpu as pltpu
from jax.sharding import PartitionSpec as P

D = 2048
NOPE = 64
ROPE = 32
VDIM = 64
TAPS = 3
NZ, NX, NY = 8, 4, 4
ROWS = 384
KVR = NOPE + ROPE + VDIM
QK = NOPE + ROPE
LOCAL = 4
BLOCKS = NZ * NX

EPSILON = 1e-06
THETA = 500000.0
NEGATIVE = -1e30
LOG2E = math.log2(math.e)
MESH = pl.DeviceIdType.MESH
VMEM = pltpu.MemorySpace.VMEM


def side(z):
    return lax.rem(lax.div(z + 1, 2), 2)


def plane(j, core):
    return 2 * j + lax.rem(j + core, 2)


def remote(src, dst, send, recv, sp, tp):
    return pltpu.make_async_remote_copy(
        src_ref=src, dst_ref=dst, send_sem=send, recv_sem=recv,
        device_id=(sp, tp), device_id_type=MESH,
    )


def attention_step(kv_ref, q_ref, m_ref, l_ref, acc_ref, block, group, active, offset):
    scale = QK ** -0.5 * LOG2E
    width = active * ROWS
    cols = slice(0, width)
    scores = []
    for g in range(group):
        keys = kv_ref[block + g, 0:QK, :].T
        value = jnp.dot(keys, q_ref[:, cols], preferred_element_type=jnp.float32)
        if offset is not None:
            start = width - ROWS
            key = lax.broadcasted_iota(jnp.int32, value.shape, 0) + (offset + g * ROWS)
            row = lax.broadcasted_iota(jnp.int32, value.shape, 1) - start
            keep = key <= row
            if start:
                keep = jnp.logical_or(keep, row < 0)
            value = jnp.where(keep, value, NEGATIVE)
        scores.append(value)
    old = m_ref[:, cols]
    top = functools.reduce(jnp.maximum, [jnp.max(v, axis=0, keepdims=True) for v in scores])
    fresh = jnp.maximum(old, top * scale)
    shrink = jnp.exp2(old - fresh)
    weights = [jnp.exp2(v * scale - fresh) for v in scores]
    m_ref[:, cols] = fresh
    l_ref[:, cols] = l_ref[:, cols] * shrink + sum(
        jnp.sum(w, axis=0, keepdims=True) for w in weights
    )
    acc_ref[:, cols] = acc_ref[:, cols] * shrink + sum(
        jnp.dot(kv_ref[block + g, QK:KVR, :], w.astype(jnp.bfloat16), preferred_element_type=jnp.float32)
        for g, w in enumerate(weights)
    )


AHEAD_A, AHEAD_B = 6, 3
AHEAD_C = 1

GROUPS = {4: 1, 3: 1, 2: 2, 1: 4}


def attend_plane(kv_ref, q_ref, state, p, core, x):
    direct = side(p) == core
    pair = lax.div(p, 2)
    later = LOCAL - pair - lax.rem(p, 2)
    for active in range(1, LOCAL + 1):
        group = GROUPS[active]

        @pl.when(jnp.logical_and(direct, pair == LOCAL - active))
        def _(active=active, group=group):
            def advance(i, carry):
                attention_step(kv_ref, q_ref, *state, p * NX + i * group, group, active,
                               (i * group - x) * ROWS)
                return carry

            lax.fori_loop(0, NX // group, advance, 0)

        @pl.when(jnp.logical_and(jnp.logical_not(direct), later == active))
        def _(active=active, group=group):
            def advance(i, carry):
                attention_step(kv_ref, q_ref, *state, p * NX + i * group, group, active, None)
                return carry

            lax.fori_loop(0, NX // group, advance, 0)


def layer_kernel(
    tokens_ref, pre_ref, taps_ref, qgain_ref, kvgain_ref, gain_ref, rope_ref, cos_ref, sin_ref,
    wo_ref, wi_ref, ws_ref, wq_ref, wkv_ref, wqup_ref, wkvup_ref, wa_ref, wc_ref,
    mixed_ref, rows_ref,
    tok, wall, wqup, wkvup, sums, squares, driven, kv_ref, q_ref, conv_ref,
    all_ref, mine_ref, wcol, wconv, convs, heads, results, logs, logs_ref, stats, m_ref, l_ref, acc_ref,
    load_sem, halo_send, halo_recv, ty_send, ty_recv, td_send, td_recv,
    kz_send, kz_recv, qz_send, qz_recv, x_send, x_recv, d_send, d_recv,
    wa_send, wa_recv, wc_send, wc_recv, cy_send, cy_recv, cd_send, cd_recv,
    rz_send, rz_recv, lz_send, lz_recv, hy_send, hy_recv, hd_send, hd_recv, s_send, s_recv,
):
    sp = lax.axis_index("sp")
    tp = lax.axis_index("tp")
    z, x = lax.div(sp, NX), lax.rem(sp, NX)
    core, y = lax.rem(tp, 2), lax.div(tp, 2)
    other = 1 - core
    mate = tp + 1 - 2 * core
    xp, xm, xf = (lax.rem(x + k, NX) for k in (1, NX - 1, 2))
    up, down, far = (lax.rem(y + k, NY) * 2 + core for k in (1, NY - 1, 2))
    flip = other - core
    to_core = side(z)
    owner = lax.div(z, LOCAL)
    half = KVR // 2
    n_tp = 2 * NY

    peers = [(lax.rem(z + k, NZ) * NX + x, 2 * y + c) for k in range(1, NZ) for c in (0, 1)]
    peers += [(z * NX + xp, tp), (z * NX + xm, tp)]
    peers += [(lax.rem(sp + k, BLOCKS), tp) for k in (1, BLOCKS - 1)]
    peers += [(sp, lax.rem(tp + k, n_tp)) for k in range(1, n_tp)]

    edges = [0]
    for ref in (wkv_ref, wq_ref, wo_ref, wi_ref, ws_ref):
        edges.append(edges[-1] + ref.shape[1])
    loads = [
        pltpu.make_async_copy(ref, wall.at[:, pl.ds(edges[i], ref.shape[1])], load_sem.at[i])
        for i, ref in enumerate((wkv_ref, wq_ref, wo_ref, wi_ref, ws_ref))
    ]
    loads += [
        pltpu.make_async_copy(wkvup_ref, wkvup, load_sem.at[5]),
        pltpu.make_async_copy(wqup_ref, wqup, load_sem.at[6]),
    ]
    for c in loads:
        c.start()
    barrier = pltpu.get_barrier_semaphore()
    for peer in peers:
        pl.semaphore_signal(barrier, inc=1, device_id=peer, device_id_type=MESH)
    pad = jnp.zeros((128 - ROPE, rope_ref.shape[1]), jnp.float32)
    wall[:, pl.ds(edges[-1], 128)] = (
        jnp.concatenate([rope_ref[...].astype(jnp.float32), pad], axis=0).T.astype(jnp.bfloat16)
    )
    pl.semaphore_wait(barrier, len(peers))

    keep = jnp.logical_and(owner == core, to_core == core)
    own_head = z - LOCAL * core
    my_pair = lax.div(z, 2)

    def slot(ref, j):
        return ref.at[:, pl.ds(pl.multiple_of((LOCAL - 1 - j) * ROWS, ROWS), ROWS)]

    def start(src, dst, s, r, to_sp, to_tp):
        remote(src, dst, s, r, to_sp, to_tp).start()

    def recv(dst, s, r):
        remote(dst, dst, s, r, sp, mate).wait_recv()

    def sent(src, s, r):
        remote(src, src, s, r, sp, mate).wait_send()

    def leaves(h):
        return jnp.logical_not(jnp.logical_and(keep, own_head == h))

    def ring_start(source, part, y_s, y_r, d_s, d_r, rows):
        start(source, part(tp, 0, rows), y_s(0), y_r(0), sp, up)
        start(source, part(tp, 0, rows), y_s(1), y_r(1), sp, down)
        start(source, part(tp, 0, rows), d_s(0), d_r(0), sp, mate)

    def ring_middle(part, y_s, y_r, d_s, d_r, rows):
        cut = rows // 2
        recv(part(down, 0, rows), y_s(0), y_r(0))
        start(part(down, 0, cut), part(down, 0, cut), y_s(2), y_r(2), sp, up)
        start(part(down, 0, rows), part(down, 0, rows), d_s(1), d_r(1), sp, mate)
        recv(part(up, 0, rows), y_s(1), y_r(1))
        start(part(up, cut, cut), part(up, cut, cut), y_s(3), y_r(3), sp, down)
        start(part(up, 0, rows), part(up, 0, rows), d_s(2), d_r(2), sp, mate)

    def ring_end(part, y_s, y_r, d_s, d_r, rows):
        cut = rows // 2
        for k in (0, 1):
            recv(part(far, k * cut, cut), y_s(2 + k), y_r(2 + k))
            start(part(far, k * cut, cut), part(far, k * cut, cut), d_s(3 + k), d_r(3 + k), sp, mate)

    def ring_far(part, d_s, d_r, rows):
        cut = rows // 2
        for k in (0, 1):
            recv(part(far + flip, k * cut, cut), d_s(3 + k), d_r(3 + k))

    def ring_recv(part, d_s, d_r, rows):
        recv(part(mate, 0, rows), d_s(0), d_r(0))
        recv(part(down + flip, 0, rows), d_s(1), d_r(1))
        recv(part(up + flip, 0, rows), d_s(2), d_r(2))
        ring_far(part, d_s, d_r, rows)

    def ring_sent(part, y_s, y_r, d_s, d_r, rows):
        cut = rows // 2
        for k in (0, 1):
            sent(part(tp, 0, rows), y_s(k), y_r(k))
            sent(part(tp, 0, cut), y_s(2 + k), y_r(2 + k))
            sent(part(tp, 0, cut), d_s(3 + k), d_r(3 + k))
        for k in (0, 1, 2):
            sent(part(tp, 0, rows), d_s(k), d_r(k))

    part_width = tokens_ref.shape[1]

    def token_part(owner_tp, first=0, count=ROWS):
        return tok.at[pl.ds(first, count), pl.ds(pl.multiple_of(owner_tp * part_width, part_width), part_width)]

    tok_sems = [lambda k, ref=ref: ref.at[k] for ref in (ty_send, ty_recv, td_send, td_recv)]
    ring_start(tokens_ref, token_part, *tok_sems, ROWS)
    tok[:, pl.ds(pl.multiple_of(tp * part_width, part_width), part_width)] = tokens_ref[...]

    def project(chip, fresh):
        share = 2 * part_width
        cols = pl.ds(pl.multiple_of(chip * share, share), share)
        wide = tok[:, cols].astype(jnp.float32)
        part = wide * wide
        part = functools.reduce(jnp.add, [part[:, k : k + 128] for k in range(0, share, 128)])
        value = jnp.dot((wide * pre_ref[:, cols]).astype(jnp.bfloat16), wall[cols, :],
                        preferred_element_type=jnp.float32)
        squares[...] = part if fresh else squares[...] + part
        sums[...] = value if fresh else sums[...] + value

    recv(token_part(mate), td_send.at[0], td_recv.at[0])
    for c in loads[:5]:
        c.wait()
    project(y, True)
    ring_middle(token_part, *tok_sems, ROWS)
    recv(token_part(down + flip), td_send.at[1], td_recv.at[1])
    project(lax.div(down, 2), False)
    ring_end(token_part, *tok_sems, ROWS)
    recv(token_part(up + flip), td_send.at[2], td_recv.at[2])
    project(lax.div(up, 2), False)
    ring_far(token_part, tok_sems[2], tok_sems[3], ROWS)
    def rows_of(ref, index, count, first=0):
        return ref.at[pl.ds(pl.multiple_of(index, count) + first, count)]

    wa_rows, wc_rows = LOCAL * VDIM, convs.shape[0] // n_tp
    width = wcol.shape[1]

    def columns(ref, owner_tp):
        return ref.at[:, pl.ds(pl.multiple_of(owner_tp * width, width), width)]

    def conv_part(owner_tp, first=0, count=wc_rows):
        return convs.at[pl.ds(pl.multiple_of(owner_tp * wc_rows + first, 16), count)]

    for k in range(1, n_tp):
        to = lax.rem(tp + k, n_tp)
        start(columns(wa_ref, to), rows_of(wcol, tp * wa_rows, wa_rows), wa_send.at[k], wa_recv.at[k], sp, to)
        start(columns(wc_ref, to), rows_of(wconv, tp * wc_rows, wc_rows), wc_send.at[k], wc_recv.at[k], sp, to)
    own_wa = pltpu.make_async_copy(columns(wa_ref, tp), rows_of(wcol, tp * wa_rows, wa_rows), wa_send.at[0])
    own_wc = pltpu.make_async_copy(columns(wc_ref, tp), rows_of(wconv, tp * wc_rows, wc_rows), wc_send.at[0])
    own_wa.start()
    own_wc.start()
    project(lax.div(far, 2), False)
    factor = lax.rsqrt(jnp.sum(squares[...], axis=1, keepdims=True) * (1.0 / D) + EPSILON)

    def normed(first, last, gain):
        value = sums[:, first:last] * factor
        mean = jnp.sum(value * value, axis=1, keepdims=True) * (1.0 / (last - first))
        return (value * lax.rsqrt(mean + EPSILON) * gain).astype(jnp.bfloat16)

    cosine, sine = cos_ref[...], sin_ref[...]

    def rotate(first, second):
        return jnp.concatenate(
            [first * cosine - second * sine, second * cosine + first * sine], axis=0
        ).astype(jnp.bfloat16)

    def plane_at(i):
        step = lax.div(i + 1, 2)
        return lax.rem(z + jnp.where(lax.rem(i, 2) == 1, step, NZ - step), NZ)

    def to_planes(send):
        for i in range(NZ):
            target = plane_at(jnp.int32(i))

            @pl.when(jnp.logical_and(lax.div(target, LOCAL) == core, leaves(target - LOCAL * core)))
            def _(target=target):
                send(target - LOCAL * core, target * NX + x, 2 * y + to_core)

    def send_keys(h, to_sp, to_tp):
        start(kv_ref.at[h], all_ref.at[sp], kz_send.at[h], kz_recv.at[my_pair], to_sp, to_tp)

    def send_queries(h, to_sp, to_tp):
        start(q_ref.at[h], slot(mine_ref, my_pair), qz_send.at[h], qz_recv.at[my_pair], to_sp, to_tp)

    loads[6].wait()
    q_gain = jnp.concatenate([qgain_ref[k : k + 1, :] for k in range(qgain_ref.shape[0])], axis=1)
    query = jnp.dot(normed(edges[1], edges[2], q_gain), wqup[...], preferred_element_type=jnp.float32).T
    for h in range(LOCAL):
        first = h * QK
        q_ref[h, 0:NOPE] = query[first : first + NOPE].astype(jnp.bfloat16)
        q_ref[h, NOPE:QK] = rotate(query[first + NOPE : first + NOPE + ROPE // 2],
                                   query[first + NOPE + ROPE // 2 : first + QK])
    to_planes(send_queries)

    loads[5].wait()
    keyvals = jnp.dot(normed(edges[0], edges[1], kvgain_ref[...]), wkvup[...], preferred_element_type=jnp.float32).T
    turn = (sums[:, edges[-1] : edges[-1] + 128] * factor).T
    rope_key = rotate(turn[: ROPE // 2], turn[ROPE // 2 : ROPE])
    for h in range(LOCAL):
        first = h * (NOPE + VDIM)
        kv_ref[h, 0:NOPE] = keyvals[first : first + NOPE].astype(jnp.bfloat16)
        kv_ref[h, NOPE:QK] = rope_key
        kv_ref[h, QK:KVR] = keyvals[first + NOPE : first + NOPE + VDIM].astype(jnp.bfloat16)
    to_planes(send_keys)
    for h in range(LOCAL):
        @pl.when(jnp.logical_not(leaves(h)))
        def _(h=h):
            all_ref[sp] = kv_ref[h]
            mine_ref[:, pl.ds(pl.multiple_of((LOCAL - 1 - my_pair) * ROWS, ROWS), ROWS)] = q_ref[h]

    outer, inner, source = (
        (sums[:, edges[k] : edges[k + 1]] * factor).astype(jnp.bfloat16) for k in (2, 3, 4)
    )
    driven[pl.ds(16, ROWS), :] = (inner.astype(jnp.float32) * source.astype(jnp.float32)).astype(jnp.bfloat16)

    @pl.when(sp < BLOCKS - 1)
    def _():
        start(driven.at[pl.ds(ROWS + 8, 8)], driven.at[pl.ds(8, 8)], halo_send, halo_recv, sp + 1, tp)

    @pl.when(sp == 0)
    def _():
        driven[pl.ds(8, 8), :] = jnp.zeros((8, driven.shape[1]), jnp.bfloat16)

    @pl.when(sp > 0)
    def _():
        recv(driven.at[pl.ds(8, 8)], halo_send, halo_recv)

    extended = driven[pl.ds(8, ROWS + 8), :].astype(jnp.float32)
    taps = taps_ref[...].astype(jnp.float32)
    convolved = functools.reduce(
        jnp.add,
        [taps[k : k + 1] * extended[9 - TAPS + k : 9 - TAPS + k + ROWS] for k in range(TAPS)],
    )
    conv_ref[...] = (outer.astype(jnp.float32) * convolved).T.astype(jnp.bfloat16)

    conv_sems = [lambda k, ref=ref: ref.at[k] for ref in (cy_send, cy_recv, cd_send, cd_recv)]
    ring_start(conv_ref, conv_part, *conv_sems, wc_rows)
    convs[pl.ds(pl.multiple_of(tp * wc_rows, wc_rows), wc_rows), :] = conv_ref[...]

    m_ref[...] = jnp.full_like(m_ref, NEGATIVE)
    l_ref[...] = jnp.zeros_like(l_ref)
    acc_ref[...] = jnp.zeros_like(acc_ref)

    def z_wait(j, dst, s, r):
        @pl.when(jnp.logical_not(jnp.logical_and(keep, plane(j, core) == z)))
        def _():
            recv(dst, s, r)

    def stage_a(p):
        @pl.when(side(p) == core)
        def _():
            j = lax.div(p, 2)
            block = all_ref.at[p * NX + x]
            z_wait(j, block, kz_send.at[0], kz_recv.at[j])
            start(block, block, x_send.at[j, 0], x_recv.at[j, 0], z * NX + xp, tp)
            start(block, block, x_send.at[j, 1], x_recv.at[j, 1], z * NX + xm, tp)
            start(block, block, d_send.at[j, 0], d_recv.at[j, 0], sp, mate)

    def stage_b(p):
        @pl.when(side(p) == core)
        def _():
            j = lax.div(p, 2)
            low, high = all_ref.at[p * NX + xm], all_ref.at[p * NX + xp]
            recv(low, x_send.at[j, 0], x_recv.at[j, 0])
            part = all_ref.at[p * NX + xm, pl.ds(0, half)]
            start(part, part, x_send.at[j, 2], x_recv.at[j, 2], z * NX + xp, tp)
            start(low, low, d_send.at[j, 1], d_recv.at[j, 1], sp, mate)
            recv(high, x_send.at[j, 1], x_recv.at[j, 1])
            part = all_ref.at[p * NX + xp, pl.ds(half, half)]
            start(part, part, x_send.at[j, 3], x_recv.at[j, 3], z * NX + xm, tp)
            start(high, high, d_send.at[j, 2], d_recv.at[j, 2], sp, mate)

    def stage_c(p):
        j = lax.div(p, 2)
        parts = [all_ref.at[p * NX + xf, pl.ds(k * half, half)] for k in (0, 1)]

        @pl.when(side(p) == core)
        def _():
            for k in (0, 1):
                recv(parts[k], x_send.at[j, 2 + k], x_recv.at[j, 2 + k])
                start(parts[k], parts[k], d_send.at[j, 3 + k], d_recv.at[j, 3 + k], sp, mate)

    def stage_d(p):
        j = lax.div(p, 2)
        parts = [all_ref.at[p * NX + xf, pl.ds(k * half, half)] for k in (0, 1)]

        @pl.when(side(p) != core)
        def _():
            for k, column in enumerate((x, xm, xp)):
                recv(all_ref.at[p * NX + column], d_send.at[j, k], d_recv.at[j, k])
            for k in (0, 1):
                recv(parts[k], d_send.at[j, 3 + k], d_recv.at[j, 3 + k])

    for i in range(AHEAD_A):
        stage_a(plane_at(jnp.int32(i)))
        if 0 <= i + AHEAD_B - AHEAD_A:
            stage_b(plane_at(jnp.int32(i + AHEAD_B - AHEAD_A)))
    for i in range(AHEAD_C):
        stage_c(plane_at(jnp.int32(i)))
    for j in range(LOCAL):
        z_wait(j, slot(mine_ref, j), qz_send.at[0], qz_recv.at[j])

    def work(i, carry):
        @pl.when(i + AHEAD_A < NZ)
        def _():
            stage_a(plane_at(i + AHEAD_A))

        @pl.when(i + AHEAD_B < NZ)
        def _():
            stage_b(plane_at(i + AHEAD_B))

        @pl.when(i == NZ - 2)
        def _():
            ring_middle(conv_part, *conv_sems, wc_rows)

        @pl.when(i + AHEAD_C < NZ)
        def _():
            stage_c(plane_at(i + AHEAD_C))

        p = plane_at(i)
        stage_d(p)
        attend_plane(all_ref, mine_ref, (m_ref, l_ref, acc_ref), p, core, x)
        return carry

    lax.fori_loop(0, NZ, work, 0)

    total = m_ref[...] * (1.0 / LOG2E) + jnp.log(l_ref[...])
    scaled = acc_ref[...] * (1.0 / l_ref[...])
    to = 2 * y + owner

    def head_rows(owner_tp, h, first=0, count=VDIM):
        return heads.at[pl.ds(pl.multiple_of((owner_tp * LOCAL + h) * VDIM + first, 16), count)]

    head = lax.rem(z, LOCAL)
    for j in range(LOCAL):
        cols = slice((LOCAL - 1 - j) * ROWS, (LOCAL - j) * ROWS)
        results[j] = scaled[:, cols].astype(jnp.bfloat16)
        logs[j] = jnp.broadcast_to(total[:, cols], logs.shape[1:])

    def stays(j):
        return jnp.logical_and(keep, plane(j, core) == z)

    for j in range(LOCAL):
        @pl.when(jnp.logical_not(stays(j)))
        def _(j=j):
            start(results.at[j], head_rows(to, head), rz_send.at[j], rz_recv.at[head], plane(j, core) * NX + x, to)
            start(logs.at[j], logs_ref.at[head], lz_send.at[j], lz_recv.at[head], plane(j, core) * NX + x, to)
    for j in range(LOCAL):
        @pl.when(stays(j))
        def _(j=j):
            heads[pl.ds(pl.multiple_of((to * LOCAL + head) * VDIM, VDIM), VDIM), :] = results[j]
            logs_ref[head] = logs[j]

    ring_end(conv_part, *conv_sems, wc_rows)
    ring_recv(conv_part, conv_sems[2], conv_sems[3], wc_rows)
    own_wc.wait()
    own_wa.wait()
    for k in range(1, n_tp):
        source = lax.rem(tp + n_tp - k, n_tp)
        recv(rows_of(wconv, source * wc_rows, wc_rows), wc_send.at[k], wc_recv.at[k])
        recv(rows_of(wcol, source * wa_rows, wa_rows), wa_send.at[k], wa_recv.at[k])
    turned = (((0,), (0,)), ((), ()))
    projected = lax.dot_general(convs[...], wconv[...], turned, preferred_element_type=jnp.float32)

    def here(h):
        return jnp.logical_and(keep, LOCAL * core + h == z)

    def head_ring(h):
        return (
            lambda owner_tp, first, count: head_rows(owner_tp, h, first, count),
            *[lambda k, ref=ref: ref.at[h, k] for ref in (hy_send, hy_recv, hd_send, hd_recv)],
            VDIM,
        )

    rings = [head_ring(h) for h in range(LOCAL)]
    for h in range(LOCAL):
        mine = head_rows(tp, h)

        @pl.when(jnp.logical_not(here(h)))
        def _(h=h, mine=mine):
            recv(mine, rz_send.at[h], rz_recv.at[h])

        part, y_s, y_r, d_s, d_r, rows = rings[h]
        ring_start(mine, part, y_s, y_r, d_s, d_r, rows)
        if h:
            ring_middle(*rings[h - 1])
    ring_middle(*rings[LOCAL - 1])

    def product(chip):
        rows = pl.ds(pl.multiple_of(chip * 2 * wa_rows, 2 * wa_rows), 2 * wa_rows)
        return lax.dot_general(heads[rows, :], wcol[rows, :], turned, preferred_element_type=jnp.float32)

    def other_core(owner_tp, index):
        for part, _, _, d_s, d_r, rows in rings:
            recv(part(owner_tp, 0, rows), d_s(index), d_r(index))

    other_core(mate, 0)
    projected = projected + product(y)
    for ring in rings:
        ring_end(*ring)
    other_core(down + flip, 1)
    projected = projected + product(lax.div(down, 2))
    other_core(up + flip, 2)
    projected = projected + product(lax.div(up, 2))
    for part, _, _, d_s, d_r, rows in rings:
        ring_far(part, d_s, d_r, rows)
    projected = projected + product(lax.div(far, 2))

    squares = projected * projected
    lanes = width // 2
    column = jnp.sum((squares[:, :lanes] + squares[:, lanes:]).T, axis=0, keepdims=True)
    stats[tp] = jnp.broadcast_to(column, stats.shape[1:])
    for k in range(1, n_tp):
        start(stats.at[tp], stats.at[tp], s_send.at[k], s_recv.at[k], sp, lax.rem(tp + k, n_tp))
    for k in range(1, n_tp):
        recv(stats.at[lax.rem(tp + n_tp - k, n_tp)], s_send.at[k], s_recv.at[k])
    summed = functools.reduce(jnp.add, [stats[t, 0:1, :] for t in range(n_tp)])
    norm = lax.rsqrt(summed * (1.0 / D) + EPSILON)
    norm = jnp.broadcast_to(norm, (lanes, ROWS)).T
    for k in (0, 1):
        cols = slice(k * lanes, (k + 1) * lanes)
        mixed_ref[:, cols] = (projected[:, cols] * norm * gain_ref[:, cols]).astype(jnp.bfloat16)

    @pl.when(sp < BLOCKS - 1)
    def _():
        sent(driven.at[pl.ds(8, 8)], halo_send, halo_recv)

    ring_sent(token_part, *tok_sems, ROWS)
    for h in range(LOCAL):
        @pl.when(leaves(h))
        def _(h=h):
            sent(q_ref.at[h], qz_send.at[h], qz_recv.at[h])
            sent(kv_ref.at[h], kz_send.at[h], kz_recv.at[h])
    for j in range(LOCAL):
        block = all_ref.at[0]
        part = all_ref.at[0, pl.ds(0, half)]
        for k in (0, 1):
            sent(block, x_send.at[j, k], x_recv.at[j, k])
            sent(part, x_send.at[j, 2 + k], x_recv.at[j, 2 + k])
            sent(part, d_send.at[j, 3 + k], d_recv.at[j, 3 + k])
        for k in (0, 1, 2):
            sent(block, d_send.at[j, k], d_recv.at[j, k])

        @pl.when(jnp.logical_not(stays(j)))
        def _(j=j):
            sent(results.at[j], rz_send.at[j], rz_recv.at[j])
            sent(logs.at[j], lz_send.at[j], lz_recv.at[j])

        @pl.when(jnp.logical_not(here(j)))
        def _(j=j):
            recv(logs_ref.at[j], lz_send.at[j], lz_recv.at[j])

        rows_ref[j : j + 1, :] = logs_ref[j, 0:1, :]
        ring_sent(*head_ring(j))
    ring_sent(conv_part, *conv_sems, wc_rows)
    for k in range(1, n_tp):
        sent(rows_of(wcol, 0, wa_rows), wa_send.at[k], wa_recv.at[k])
        sent(rows_of(wconv, 0, wc_rows), wc_send.at[k], wc_recv.at[k])
        sent(stats.at[0], s_send.at[k], s_recv.at[k])


def layer(tokens, small, matrices):
    dma = pltpu.SemaphoreType.DMA
    wa, wc = matrices[-2:]
    wqup, wkvup = matrices[5:7]
    wa_rows, wc_rows = wa.shape[0], wc.shape[0]
    n_tp = 2 * NY
    width = wa.shape[1] // n_tp
    bf16, f32 = jnp.bfloat16, jnp.float32
    total = sum(m.shape[1] for m in matrices[:5]) + 128
    sems = [dma((7,)), dma, dma]
    for shape in ((4,), (5,), (4,), (4,), (4, 4), (4, 5), (8,), (8,), (4,), (5,), (4,), (4,), (4, 4), (4, 5), (8,)):
        sems += [dma(shape), dma(shape)]
    return pl.pallas_call(
        layer_kernel,
        out_shape=(
            jax.ShapeDtypeStruct((ROWS, width), bf16),
            jax.ShapeDtypeStruct((LOCAL, ROWS), f32),
        ),
        in_specs=[pl.BlockSpec(memory_space=VMEM)] * (1 + len(small))
        + [pl.BlockSpec(memory_space=pl.ANY)] * len(matrices),
        out_specs=(pl.BlockSpec(memory_space=VMEM),) * 2,
        scratch_shapes=[
            pltpu.VMEM((ROWS, D), bf16),
            pltpu.VMEM((D, total), bf16),
            pltpu.VMEM(wqup.shape, bf16),
            pltpu.VMEM(wkvup.shape, bf16),
            pltpu.VMEM((ROWS, total), f32),
            pltpu.VMEM((ROWS, 128), f32),
            pltpu.VMEM((ROWS + 16, wc_rows), bf16),
            pltpu.VMEM((LOCAL, KVR, ROWS), bf16),
            pltpu.VMEM((LOCAL, QK, ROWS), bf16),
            pltpu.VMEM((wc_rows, ROWS), bf16),
            pltpu.VMEM((BLOCKS, KVR, ROWS), bf16),
            pltpu.VMEM((QK, LOCAL * ROWS), bf16),
            pltpu.VMEM((wa_rows * n_tp, width), bf16),
            pltpu.VMEM((wc_rows * n_tp, width), bf16),
            pltpu.VMEM((wc_rows * n_tp, ROWS), bf16),
            pltpu.VMEM((wa_rows * n_tp, ROWS), bf16),
            pltpu.VMEM((LOCAL, VDIM, ROWS), bf16),
            pltpu.VMEM((LOCAL, 8, ROWS), f32),
            pltpu.VMEM((LOCAL, 8, ROWS), f32),
            pltpu.VMEM((n_tp, 8, ROWS), f32),
            pltpu.VMEM((1, LOCAL * ROWS), f32),
            pltpu.VMEM((1, LOCAL * ROWS), f32),
            pltpu.VMEM((VDIM, LOCAL * ROWS), f32),
        ] + sems,
        compiler_params=pltpu.CompilerParams(
            collective_id=1, has_side_effects=True, vmem_limit_bytes=60 * 2**20,
        ),
        name="layer_rest",
    )(tokens, *small, *matrices)


def rotation(positions, width):
    freqs = THETA ** (-jnp.arange(0, width, 2, dtype=jnp.float32) / width)
    angles = freqs[:, None] * positions.astype(jnp.float32)[None, :]
    return (jnp.cos(angles), jnp.sin(angles))


def body(
    tokens,
    pre_gain,
    outer_gate_weight,
    inner_gate_weight,
    source_weight,
    conv_taps,
    q_down_weight,
    q_norm_gain,
    q_up_weight,
    kv_down_weight,
    rope_key_weight,
    kv_norm_gain,
    kv_up_weight,
    attn_out_weight,
    conv_out_weight,
    post_gain,
):
    token_rows = tokens.shape[0]
    query_pos = lax.axis_index("sp") * token_rows + jnp.arange(token_rows, dtype=jnp.int32)
    cosine, sine = rotation(query_pos, ROPE)
    small = (
        pre_gain[None, :], conv_taps, q_norm_gain.reshape(-1, 128), kv_norm_gain[None, :], post_gain[None, :],
        rope_key_weight.T, cosine, sine,
    )
    matrices = (
        outer_gate_weight, inner_gate_weight, source_weight, q_down_weight, kv_down_weight,
        q_up_weight, kv_up_weight, attn_out_weight, conv_out_weight,
    )
    return layer(tokens, small, matrices)


def solution(mesh):
    placed = (
        P("sp", "tp"),
        P(),
        P(None, "tp"),
        P(None, "tp"),
        P(None, "tp"),
        P(None, "tp"),
        P(),
        P(),
        P(None, "tp"),
        P(),
        P(),
        P(),
        P(None, "tp"),
        P("tp", None),
        P("tp", None),
        P("tp"),
    )
    return jax.shard_map(
        body, mesh=mesh, in_specs=placed, out_specs=(P("sp", "tp"), P("tp", "sp")), check_vma=False
    )
```

```python
import functools
import math

import jax
import jax.numpy as jnp
from jax import lax
from jax.experimental import pallas as pl
from jax.experimental.pallas import tpu as pltpu
from jax.sharding import PartitionSpec as P

D = 2048
NOPE = 64
ROPE = 32
VDIM = 64
TAPS = 3
NZ, NX, NY = 8, 4, 4
ROWS = 384
KVR = NOPE + ROPE + VDIM
QK = NOPE + ROPE
LOCAL = 4
BLOCKS = NZ * NX

EPSILON = 1e-06
THETA = 500000.0
NEGATIVE = -1e30
LOG2E = math.log2(math.e)
MESH = pl.DeviceIdType.MESH
VMEM = pltpu.MemorySpace.VMEM


def side(z):
    return lax.rem(lax.div(z + 1, 2), 2)


def plane(j, core):
    return 2 * j + lax.rem(j + core, 2)


def remote(src, dst, send, recv, sp, tp):
    return pltpu.make_async_remote_copy(
        src_ref=src, dst_ref=dst, send_sem=send, recv_sem=recv,
        device_id=(sp, tp), device_id_type=MESH,
    )


def attention_step(kv_ref, q_ref, m_ref, l_ref, acc_ref, block, group, active, offset):
    scale = QK ** -0.5 * LOG2E
    width = active * ROWS
    cols = slice(0, width)
    scores = []
    for g in range(group):
        keys = kv_ref[block + g, 0:QK, :].T
        value = jnp.dot(keys, q_ref[:, cols], preferred_element_type=jnp.float32)
        if offset is not None:
            start = width - ROWS
            key = lax.broadcasted_iota(jnp.int32, value.shape, 0) + (offset + g * ROWS)
            row = lax.broadcasted_iota(jnp.int32, value.shape, 1) - start
            keep = key <= row
            if start:
                keep = jnp.logical_or(keep, row < 0)
            value = jnp.where(keep, value, NEGATIVE)
        scores.append(value)
    old = m_ref[:, cols]
    top = functools.reduce(jnp.maximum, [jnp.max(v, axis=0, keepdims=True) for v in scores])
    fresh = jnp.maximum(old, top * scale)
    shrink = jnp.exp2(old - fresh)
    weights = [jnp.exp2(v * scale - fresh) for v in scores]
    m_ref[:, cols] = fresh
    l_ref[:, cols] = l_ref[:, cols] * shrink + sum(
        jnp.sum(w, axis=0, keepdims=True) for w in weights
    )
    acc_ref[:, cols] = acc_ref[:, cols] * shrink + sum(
        jnp.dot(kv_ref[block + g, QK:KVR, :], w.astype(jnp.bfloat16), preferred_element_type=jnp.float32)
        for g, w in enumerate(weights)
    )


AHEAD_A, AHEAD_B = 6, 3
AHEAD_C = 1

GROUPS = {4: 1, 3: 1, 2: 2, 1: 4}


def attend_plane(kv_ref, q_ref, state, p, core, x):
    direct = side(p) == core
    pair = lax.div(p, 2)
    later = LOCAL - pair - lax.rem(p, 2)
    for active in range(1, LOCAL + 1):
        group = GROUPS[active]

        @pl.when(jnp.logical_and(direct, pair == LOCAL - active))
        def _(active=active, group=group):
            def advance(i, carry):
                attention_step(kv_ref, q_ref, *state, p * NX + i * group, group, active,
                               (i * group - x) * ROWS)
                return carry

            lax.fori_loop(0, NX // group, advance, 0)

        @pl.when(jnp.logical_and(jnp.logical_not(direct), later == active))
        def _(active=active, group=group):
            def advance(i, carry):
                attention_step(kv_ref, q_ref, *state, p * NX + i * group, group, active, None)
                return carry

            lax.fori_loop(0, NX // group, advance, 0)


def layer_kernel(
    tokens_ref, pre_ref, taps_ref, qgain_ref, kvgain_ref, gain_ref, rope_ref, cos_ref, sin_ref,
    wo_ref, wi_ref, ws_ref, wq_ref, wkv_ref, wqup_ref, wkvup_ref, wa_ref, wc_ref,
    mixed_ref, rows_ref,
    tok, wall, wqup, wkvup, sums, squares, driven, kv_ref, q_ref, conv_ref,
    all_ref, mine_ref, wcol, wconv, convs, heads, results, logs, logs_ref, stats, m_ref, l_ref, acc_ref,
    load_sem, halo_send, halo_recv, ty_send, ty_recv, td_send, td_recv,
    kz_send, kz_recv, qz_send, qz_recv, x_send, x_recv, d_send, d_recv,
    wa_send, wa_recv, wc_send, wc_recv, cy_send, cy_recv, cd_send, cd_recv,
    rz_send, rz_recv, lz_send, lz_recv, hy_send, hy_recv, hd_send, hd_recv, s_send, s_recv,
):
    sp = lax.axis_index("sp")
    tp = lax.axis_index("tp")
    z, x = lax.div(sp, NX), lax.rem(sp, NX)
    core, y = lax.rem(tp, 2), lax.div(tp, 2)
    other = 1 - core
    mate = tp + 1 - 2 * core
    xp, xm, xf = (lax.rem(x + k, NX) for k in (1, NX - 1, 2))
    up, down, far = (lax.rem(y + k, NY) * 2 + core for k in (1, NY - 1, 2))
    flip = other - core
    to_core = side(z)
    owner = lax.div(z, LOCAL)
    half = KVR // 2
    n_tp = 2 * NY

    peers = [(lax.rem(z + k, NZ) * NX + x, 2 * y + c) for k in range(1, NZ) for c in (0, 1)]
    peers += [(z * NX + xp, tp), (z * NX + xm, tp)]
    peers += [(lax.rem(sp + k, BLOCKS), tp) for k in (1, BLOCKS - 1)]
    peers += [(sp, lax.rem(tp + k, n_tp)) for k in range(1, n_tp)]

    edges = [0]
    for ref in (wkv_ref, wq_ref, wo_ref, wi_ref, ws_ref):
        edges.append(edges[-1] + ref.shape[1])
    loads = [
        pltpu.make_async_copy(ref, wall.at[:, pl.ds(edges[i], ref.shape[1])], load_sem.at[i])
        for i, ref in enumerate((wkv_ref, wq_ref, wo_ref, wi_ref, ws_ref))
    ]
    loads += [
        pltpu.make_async_copy(wkvup_ref, wkvup, load_sem.at[5]),
        pltpu.make_async_copy(wqup_ref, wqup, load_sem.at[6]),
    ]
    for c in loads:
        c.start()
    barrier = pltpu.get_barrier_semaphore()
    for peer in peers:
        pl.semaphore_signal(barrier, inc=1, device_id=peer, device_id_type=MESH)
    pad = jnp.zeros((128 - ROPE, rope_ref.shape[1]), jnp.float32)
    wall[:, pl.ds(edges[-1], 128)] = (
        jnp.concatenate([rope_ref[...].astype(jnp.float32), pad], axis=0).T.astype(jnp.bfloat16)
    )
    pl.semaphore_wait(barrier, len(peers))

    keep = jnp.logical_and(owner == core, to_core == core)
    own_head = z - LOCAL * core
    my_pair = lax.div(z, 2)

    def slot(ref, j):
        return ref.at[:, pl.ds(pl.multiple_of((LOCAL - 1 - j) * ROWS, ROWS), ROWS)]

    def start(src, dst, s, r, to_sp, to_tp):
        remote(src, dst, s, r, to_sp, to_tp).start()

    def recv(dst, s, r):
        remote(dst, dst, s, r, sp, mate).wait_recv()

    def sent(src, s, r):
        remote(src, src, s, r, sp, mate).wait_send()

    def leaves(h):
        return jnp.logical_not(jnp.logical_and(keep, own_head == h))

    def ring_start(source, part, y_s, y_r, d_s, d_r, rows):
        start(source, part(tp, 0, rows), y_s(0), y_r(0), sp, up)
        start(source, part(tp, 0, rows), y_s(1), y_r(1), sp, down)
        start(source, part(tp, 0, rows), d_s(0), d_r(0), sp, mate)

    def ring_middle(part, y_s, y_r, d_s, d_r, rows):
        cut = rows // 2
        recv(part(down, 0, rows), y_s(0), y_r(0))
        start(part(down, 0, cut), part(down, 0, cut), y_s(2), y_r(2), sp, up)
        start(part(down, 0, rows), part(down, 0, rows), d_s(1), d_r(1), sp, mate)
        recv(part(up, 0, rows), y_s(1), y_r(1))
        start(part(up, cut, cut), part(up, cut, cut), y_s(3), y_r(3), sp, down)
        start(part(up, 0, rows), part(up, 0, rows), d_s(2), d_r(2), sp, mate)

    def ring_end(part, y_s, y_r, d_s, d_r, rows):
        cut = rows // 2
        for k in (0, 1):
            recv(part(far, k * cut, cut), y_s(2 + k), y_r(2 + k))
            start(part(far, k * cut, cut), part(far, k * cut, cut), d_s(3 + k), d_r(3 + k), sp, mate)

    def ring_far(part, d_s, d_r, rows):
        cut = rows // 2
        for k in (0, 1):
            recv(part(far + flip, k * cut, cut), d_s(3 + k), d_r(3 + k))

    def ring_recv(part, d_s, d_r, rows):
        recv(part(mate, 0, rows), d_s(0), d_r(0))
        recv(part(down + flip, 0, rows), d_s(1), d_r(1))
        recv(part(up + flip, 0, rows), d_s(2), d_r(2))
        ring_far(part, d_s, d_r, rows)

    def ring_sent(part, y_s, y_r, d_s, d_r, rows):
        cut = rows // 2
        for k in (0, 1):
            sent(part(tp, 0, rows), y_s(k), y_r(k))
            sent(part(tp, 0, cut), y_s(2 + k), y_r(2 + k))
            sent(part(tp, 0, cut), d_s(3 + k), d_r(3 + k))
        for k in (0, 1, 2):
            sent(part(tp, 0, rows), d_s(k), d_r(k))

    part_width = tokens_ref.shape[1]

    def token_part(owner_tp, first=0, count=ROWS):
        return tok.at[pl.ds(first, count), pl.ds(pl.multiple_of(owner_tp * part_width, part_width), part_width)]

    tok_sems = [lambda k, ref=ref: ref.at[k] for ref in (ty_send, ty_recv, td_send, td_recv)]
    ring_start(tokens_ref, token_part, *tok_sems, ROWS)
    tok[:, pl.ds(pl.multiple_of(tp * part_width, part_width), part_width)] = tokens_ref[...]

    def project(chip, fresh):
        share = 2 * part_width
        cols = pl.ds(pl.multiple_of(chip * share, share), share)
        wide = tok[:, cols].astype(jnp.float32)
        part = wide * wide
        part = functools.reduce(jnp.add, [part[:, k : k + 128] for k in range(0, share, 128)])
        value = jnp.dot((wide * pre_ref[:, cols]).astype(jnp.bfloat16), wall[cols, :],
                        preferred_element_type=jnp.float32)
        squares[...] = part if fresh else squares[...] + part
        sums[...] = value if fresh else sums[...] + value

    recv(token_part(mate), td_send.at[0], td_recv.at[0])
    for c in loads[:5]:
        c.wait()
    project(y, True)
    ring_middle(token_part, *tok_sems, ROWS)
    recv(token_part(down + flip), td_send.at[1], td_recv.at[1])
    project(lax.div(down, 2), False)
    ring_end(token_part, *tok_sems, ROWS)
    recv(token_part(up + flip), td_send.at[2], td_recv.at[2])
    project(lax.div(up, 2), False)
    ring_far(token_part, tok_sems[2], tok_sems[3], ROWS)
    def rows_of(ref, index, count, first=0):
        return ref.at[pl.ds(pl.multiple_of(index, count) + first, count)]

    wa_rows, wc_rows = LOCAL * VDIM, convs.shape[0] // n_tp
    width = wcol.shape[1]

    def columns(ref, owner_tp):
        return ref.at[:, pl.ds(pl.multiple_of(owner_tp * width, width), width)]

    def conv_part(owner_tp, first=0, count=wc_rows):
        return convs.at[pl.ds(pl.multiple_of(owner_tp * wc_rows + first, 16), count)]

    for k in range(1, n_tp):
        to = lax.rem(tp + k, n_tp)
        start(columns(wa_ref, to), rows_of(wcol, tp * wa_rows, wa_rows), wa_send.at[k], wa_recv.at[k], sp, to)
        start(columns(wc_ref, to), rows_of(wconv, tp * wc_rows, wc_rows), wc_send.at[k], wc_recv.at[k], sp, to)
    own_wa = pltpu.make_async_copy(columns(wa_ref, tp), rows_of(wcol, tp * wa_rows, wa_rows), wa_send.at[0])
    own_wc = pltpu.make_async_copy(columns(wc_ref, tp), rows_of(wconv, tp * wc_rows, wc_rows), wc_send.at[0])
    own_wa.start()
    own_wc.start()
    project(lax.div(far, 2), False)
    factor = lax.rsqrt(jnp.sum(squares[...], axis=1, keepdims=True) * (1.0 / D) + EPSILON)

    def normed(first, last, gain):
        value = sums[:, first:last] * factor
        mean = jnp.sum(value * value, axis=1, keepdims=True) * (1.0 / (last - first))
        return (value * lax.rsqrt(mean + EPSILON) * gain).astype(jnp.bfloat16)

    cosine, sine = cos_ref[...], sin_ref[...]

    def rotate(first, second):
        return jnp.concatenate(
            [first * cosine - second * sine, second * cosine + first * sine], axis=0
        ).astype(jnp.bfloat16)

    def plane_at(i):
        step = lax.div(i + 1, 2)
        return lax.rem(z + jnp.where(lax.rem(i, 2) == 1, step, NZ - step), NZ)

    def to_planes(send):
        for i in range(NZ):
            target = plane_at(jnp.int32(i))

            @pl.when(jnp.logical_and(lax.div(target, LOCAL) == core, leaves(target - LOCAL * core)))
            def _(target=target):
                send(target - LOCAL * core, target * NX + x, 2 * y + to_core)

    def send_keys(h, to_sp, to_tp):
        start(kv_ref.at[h], all_ref.at[sp], kz_send.at[h], kz_recv.at[my_pair], to_sp, to_tp)

    def send_queries(h, to_sp, to_tp):
        start(q_ref.at[h], slot(mine_ref, my_pair), qz_send.at[h], qz_recv.at[my_pair], to_sp, to_tp)

    loads[6].wait()
    q_gain = jnp.concatenate([qgain_ref[k : k + 1, :] for k in range(qgain_ref.shape[0])], axis=1)
    query = jnp.dot(normed(edges[1], edges[2], q_gain), wqup[...], preferred_element_type=jnp.float32).T
    for h in range(LOCAL):
        first = h * QK
        q_ref[h, 0:NOPE] = query[first : first + NOPE].astype(jnp.bfloat16)
        q_ref[h, NOPE:QK] = rotate(query[first + NOPE : first + NOPE + ROPE // 2],
                                   query[first + NOPE + ROPE // 2 : first + QK])
    to_planes(send_queries)

    loads[5].wait()
    keyvals = jnp.dot(normed(edges[0], edges[1], kvgain_ref[...]), wkvup[...], preferred_element_type=jnp.float32).T
    turn = (sums[:, edges[-1] : edges[-1] + 128] * factor).T
    rope_key = rotate(turn[: ROPE // 2], turn[ROPE // 2 : ROPE])
    for h in range(LOCAL):
        first = h * (NOPE + VDIM)
        kv_ref[h, 0:NOPE] = keyvals[first : first + NOPE].astype(jnp.bfloat16)
        kv_ref[h, NOPE:QK] = rope_key
        kv_ref[h, QK:KVR] = keyvals[first + NOPE : first + NOPE + VDIM].astype(jnp.bfloat16)
    to_planes(send_keys)
    for h in range(LOCAL):
        @pl.when(jnp.logical_not(leaves(h)))
        def _(h=h):
            all_ref[sp] = kv_ref[h]
            mine_ref[:, pl.ds(pl.multiple_of((LOCAL - 1 - my_pair) * ROWS, ROWS), ROWS)] = q_ref[h]

    outer, inner, source = (
        (sums[:, edges[k] : edges[k + 1]] * factor).astype(jnp.bfloat16) for k in (2, 3, 4)
    )
    driven[pl.ds(16, ROWS), :] = (inner.astype(jnp.float32) * source.astype(jnp.float32)).astype(jnp.bfloat16)

    @pl.when(sp < BLOCKS - 1)
    def _():
        start(driven.at[pl.ds(ROWS + 8, 8)], driven.at[pl.ds(8, 8)], halo_send, halo_recv, sp + 1, tp)

    @pl.when(sp == 0)
    def _():
        driven[pl.ds(8, 8), :] = jnp.zeros((8, driven.shape[1]), jnp.bfloat16)

    @pl.when(sp > 0)
    def _():
        recv(driven.at[pl.ds(8, 8)], halo_send, halo_recv)

    extended = driven[pl.ds(8, ROWS + 8), :].astype(jnp.float32)
    taps = taps_ref[...].astype(jnp.float32)
    convolved = functools.reduce(
        jnp.add,
        [taps[k : k + 1] * extended[9 - TAPS + k : 9 - TAPS + k + ROWS] for k in range(TAPS)],
    )
    conv_ref[...] = (outer.astype(jnp.float32) * convolved).T.astype(jnp.bfloat16)

    conv_sems = [lambda k, ref=ref: ref.at[k] for ref in (cy_send, cy_recv, cd_send, cd_recv)]
    ring_start(conv_ref, conv_part, *conv_sems, wc_rows)
    convs[pl.ds(pl.multiple_of(tp * wc_rows, wc_rows), wc_rows), :] = conv_ref[...]

    m_ref[...] = jnp.full_like(m_ref, NEGATIVE)
    l_ref[...] = jnp.zeros_like(l_ref)
    acc_ref[...] = jnp.zeros_like(acc_ref)

    def z_wait(j, dst, s, r):
        @pl.when(jnp.logical_not(jnp.logical_and(keep, plane(j, core) == z)))
        def _():
            recv(dst, s, r)

    def stage_a(p):
        @pl.when(side(p) == core)
        def _():
            j = lax.div(p, 2)
            block = all_ref.at[p * NX + x]
            z_wait(j, block, kz_send.at[0], kz_recv.at[j])
            start(block, block, x_send.at[j, 0], x_recv.at[j, 0], z * NX + xp, tp)
            start(block, block, x_send.at[j, 1], x_recv.at[j, 1], z * NX + xm, tp)
            start(block, block, d_send.at[j, 0], d_recv.at[j, 0], sp, mate)

    def stage_b(p):
        @pl.when(side(p) == core)
        def _():
            j = lax.div(p, 2)
            low, high = all_ref.at[p * NX + xm], all_ref.at[p * NX + xp]
            recv(low, x_send.at[j, 0], x_recv.at[j, 0])
            part = all_ref.at[p * NX + xm, pl.ds(0, half)]
            start(part, part, x_send.at[j, 2], x_recv.at[j, 2], z * NX + xp, tp)
            start(low, low, d_send.at[j, 1], d_recv.at[j, 1], sp, mate)
            recv(high, x_send.at[j, 1], x_recv.at[j, 1])
            part = all_ref.at[p * NX + xp, pl.ds(half, half)]
            start(part, part, x_send.at[j, 3], x_recv.at[j, 3], z * NX + xm, tp)
            start(high, high, d_send.at[j, 2], d_recv.at[j, 2], sp, mate)

    def stage_c(p):
        j = lax.div(p, 2)
        parts = [all_ref.at[p * NX + xf, pl.ds(k * half, half)] for k in (0, 1)]

        @pl.when(side(p) == core)
        def _():
            for k in (0, 1):
                recv(parts[k], x_send.at[j, 2 + k], x_recv.at[j, 2 + k])
                start(parts[k], parts[k], d_send.at[j, 3 + k], d_recv.at[j, 3 + k], sp, mate)

    def stage_d(p):
        j = lax.div(p, 2)
        parts = [all_ref.at[p * NX + xf, pl.ds(k * half, half)] for k in (0, 1)]

        @pl.when(side(p) != core)
        def _():
            for k, column in enumerate((x, xm, xp)):
                recv(all_ref.at[p * NX + column], d_send.at[j, k], d_recv.at[j, k])
            for k in (0, 1):
                recv(parts[k], d_send.at[j, 3 + k], d_recv.at[j, 3 + k])

    for i in range(AHEAD_A):
        stage_a(plane_at(jnp.int32(i)))
        if 0 <= i + AHEAD_B - AHEAD_A:
            stage_b(plane_at(jnp.int32(i + AHEAD_B - AHEAD_A)))
    for i in range(AHEAD_C):
        stage_c(plane_at(jnp.int32(i)))
    for j in range(LOCAL):
        z_wait(j, slot(mine_ref, j), qz_send.at[0], qz_recv.at[j])

    def work(i, carry):
        @pl.when(i + AHEAD_A < NZ)
        def _():
            stage_a(plane_at(i + AHEAD_A))

        @pl.when(i + AHEAD_B < NZ)
        def _():
            stage_b(plane_at(i + AHEAD_B))

        @pl.when(i == NZ - 2)
        def _():
            ring_middle(conv_part, *conv_sems, wc_rows)

        @pl.when(i + AHEAD_C < NZ)
        def _():
            stage_c(plane_at(i + AHEAD_C))

        p = plane_at(i)
        stage_d(p)
        attend_plane(all_ref, mine_ref, (m_ref, l_ref, acc_ref), p, core, x)
        return carry

    lax.fori_loop(0, NZ, work, 0)

    total = m_ref[...] * (1.0 / LOG2E) + jnp.log(l_ref[...])
    scaled = acc_ref[...] * (1.0 / l_ref[...])
    to = 2 * y + owner

    def head_rows(owner_tp, h, first=0, count=VDIM):
        return heads.at[pl.ds(pl.multiple_of((owner_tp * LOCAL + h) * VDIM + first, 16), count)]

    head = lax.rem(z, LOCAL)
    for j in range(LOCAL):
        cols = slice((LOCAL - 1 - j) * ROWS, (LOCAL - j) * ROWS)
        results[j] = scaled[:, cols].astype(jnp.bfloat16)
        logs[j] = jnp.broadcast_to(total[:, cols], logs.shape[1:])

    def stays(j):
        return jnp.logical_and(keep, plane(j, core) == z)

    for j in range(LOCAL):
        @pl.when(jnp.logical_not(stays(j)))
        def _(j=j):
            start(results.at[j], head_rows(to, head), rz_send.at[j], rz_recv.at[head], plane(j, core) * NX + x, to)

    for j in range(LOCAL):
        @pl.when(jnp.logical_not(stays(j)))
        def _(j=j):
            start(logs.at[j], logs_ref.at[head], lz_send.at[j], lz_recv.at[head], plane(j, core) * NX + x, to)
    for j in range(LOCAL):
        @pl.when(stays(j))
        def _(j=j):
            heads[pl.ds(pl.multiple_of((to * LOCAL + head) * VDIM, VDIM), VDIM), :] = results[j]
            logs_ref[head] = logs[j]

    ring_end(conv_part, *conv_sems, wc_rows)
    ring_recv(conv_part, conv_sems[2], conv_sems[3], wc_rows)
    own_wc.wait()
    own_wa.wait()
    for k in range(1, n_tp):
        source = lax.rem(tp + n_tp - k, n_tp)
        recv(rows_of(wconv, source * wc_rows, wc_rows), wc_send.at[k], wc_recv.at[k])
        recv(rows_of(wcol, source * wa_rows, wa_rows), wa_send.at[k], wa_recv.at[k])
    turned = (((0,), (0,)), ((), ()))
    projected = lax.dot_general(convs[...], wconv[...], turned, preferred_element_type=jnp.float32)

    def here(h):
        return jnp.logical_and(keep, LOCAL * core + h == z)

    def head_ring(h):
        return (
            lambda owner_tp, first, count: head_rows(owner_tp, h, first, count),
            *[lambda k, ref=ref: ref.at[h, k] for ref in (hy_send, hy_recv, hd_send, hd_recv)],
            VDIM,
        )

    rings = [head_ring(h) for h in range(LOCAL)]
    for h in range(LOCAL):
        mine = head_rows(tp, h)

        @pl.when(jnp.logical_not(here(h)))
        def _(h=h, mine=mine):
            recv(mine, rz_send.at[h], rz_recv.at[h])

        part, y_s, y_r, d_s, d_r, rows = rings[h]
        ring_start(mine, part, y_s, y_r, d_s, d_r, rows)
        if h:
            ring_middle(*rings[h - 1])
    ring_middle(*rings[LOCAL - 1])

    def product(chip):
        rows = pl.ds(pl.multiple_of(chip * 2 * wa_rows, 2 * wa_rows), 2 * wa_rows)
        return lax.dot_general(heads[rows, :], wcol[rows, :], turned, preferred_element_type=jnp.float32)

    def other_core(owner_tp, index):
        for part, _, _, d_s, d_r, rows in rings:
            recv(part(owner_tp, 0, rows), d_s(index), d_r(index))

    other_core(mate, 0)
    projected = projected + product(y)
    for ring in rings:
        ring_end(*ring)
    other_core(down + flip, 1)
    projected = projected + product(lax.div(down, 2))
    other_core(up + flip, 2)
    projected = projected + product(lax.div(up, 2))
    for part, _, _, d_s, d_r, rows in rings:
        ring_far(part, d_s, d_r, rows)
    projected = projected + product(lax.div(far, 2))

    squares = projected * projected
    lanes = width // 2
    column = jnp.sum((squares[:, :lanes] + squares[:, lanes:]).T, axis=0, keepdims=True)
    stats[tp] = jnp.broadcast_to(column, stats.shape[1:])
    for k in range(1, n_tp):
        start(stats.at[tp], stats.at[tp], s_send.at[k], s_recv.at[k], sp, lax.rem(tp + k, n_tp))
    for k in range(1, n_tp):
        recv(stats.at[lax.rem(tp + n_tp - k, n_tp)], s_send.at[k], s_recv.at[k])
    summed = functools.reduce(jnp.add, [stats[t, 0:1, :] for t in range(n_tp)])
    norm = lax.rsqrt(summed * (1.0 / D) + EPSILON)
    norm = jnp.broadcast_to(norm, (lanes, ROWS)).T
    for k in (0, 1):
        cols = slice(k * lanes, (k + 1) * lanes)
        mixed_ref[:, cols] = (projected[:, cols] * norm * gain_ref[:, cols]).astype(jnp.bfloat16)

    @pl.when(sp < BLOCKS - 1)
    def _():
        sent(driven.at[pl.ds(8, 8)], halo_send, halo_recv)

    ring_sent(token_part, *tok_sems, ROWS)
    for h in range(LOCAL):
        @pl.when(leaves(h))
        def _(h=h):
            sent(q_ref.at[h], qz_send.at[h], qz_recv.at[h])
            sent(kv_ref.at[h], kz_send.at[h], kz_recv.at[h])
    for j in range(LOCAL):
        block = all_ref.at[0]
        part = all_ref.at[0, pl.ds(0, half)]
        for k in (0, 1):
            sent(block, x_send.at[j, k], x_recv.at[j, k])
            sent(part, x_send.at[j, 2 + k], x_recv.at[j, 2 + k])
            sent(part, d_send.at[j, 3 + k], d_recv.at[j, 3 + k])
        for k in (0, 1, 2):
            sent(block, d_send.at[j, k], d_recv.at[j, k])

        @pl.when(jnp.logical_not(stays(j)))
        def _(j=j):
            sent(results.at[j], rz_send.at[j], rz_recv.at[j])
            sent(logs.at[j], lz_send.at[j], lz_recv.at[j])

        @pl.when(jnp.logical_not(here(j)))
        def _(j=j):
            recv(logs_ref.at[j], lz_send.at[j], lz_recv.at[j])

        rows_ref[j : j + 1, :] = logs_ref[j, 0:1, :]
        ring_sent(*head_ring(j))
    ring_sent(conv_part, *conv_sems, wc_rows)
    for k in range(1, n_tp):
        sent(rows_of(wcol, 0, wa_rows), wa_send.at[k], wa_recv.at[k])
        sent(rows_of(wconv, 0, wc_rows), wc_send.at[k], wc_recv.at[k])
        sent(stats.at[0], s_send.at[k], s_recv.at[k])


def layer(tokens, small, matrices):
    dma = pltpu.SemaphoreType.DMA
    wa, wc = matrices[-2:]
    wqup, wkvup = matrices[5:7]
    wa_rows, wc_rows = wa.shape[0], wc.shape[0]
    n_tp = 2 * NY
    width = wa.shape[1] // n_tp
    bf16, f32 = jnp.bfloat16, jnp.float32
    total = sum(m.shape[1] for m in matrices[:5]) + 128
    sems = [dma((7,)), dma, dma]
    for shape in ((4,), (5,), (4,), (4,), (4, 4), (4, 5), (8,), (8,), (4,), (5,), (4,), (4,), (4, 4), (4, 5), (8,)):
        sems += [dma(shape), dma(shape)]
    return pl.pallas_call(
        layer_kernel,
        out_shape=(
            jax.ShapeDtypeStruct((ROWS, width), bf16),
            jax.ShapeDtypeStruct((LOCAL, ROWS), f32),
        ),
        in_specs=[pl.BlockSpec(memory_space=VMEM)] * (1 + len(small))
        + [pl.BlockSpec(memory_space=pl.ANY)] * len(matrices),
        out_specs=(pl.BlockSpec(memory_space=VMEM),) * 2,
        scratch_shapes=[
            pltpu.VMEM((ROWS, D), bf16),
            pltpu.VMEM((D, total), bf16),
            pltpu.VMEM(wqup.shape, bf16),
            pltpu.VMEM(wkvup.shape, bf16),
            pltpu.VMEM((ROWS, total), f32),
            pltpu.VMEM((ROWS, 128), f32),
            pltpu.VMEM((ROWS + 16, wc_rows), bf16),
            pltpu.VMEM((LOCAL, KVR, ROWS), bf16),
            pltpu.VMEM((LOCAL, QK, ROWS), bf16),
            pltpu.VMEM((wc_rows, ROWS), bf16),
            pltpu.VMEM((BLOCKS, KVR, ROWS), bf16),
            pltpu.VMEM((QK, LOCAL * ROWS), bf16),
            pltpu.VMEM((wa_rows * n_tp, width), bf16),
            pltpu.VMEM((wc_rows * n_tp, width), bf16),
            pltpu.VMEM((wc_rows * n_tp, ROWS), bf16),
            pltpu.VMEM((wa_rows * n_tp, ROWS), bf16),
            pltpu.VMEM((LOCAL, VDIM, ROWS), bf16),
            pltpu.VMEM((LOCAL, 8, ROWS), f32),
            pltpu.VMEM((LOCAL, 8, ROWS), f32),
            pltpu.VMEM((n_tp, 8, ROWS), f32),
            pltpu.VMEM((1, LOCAL * ROWS), f32),
            pltpu.VMEM((1, LOCAL * ROWS), f32),
            pltpu.VMEM((VDIM, LOCAL * ROWS), f32),
        ] + sems,
        compiler_params=pltpu.CompilerParams(
            collective_id=1, has_side_effects=True, vmem_limit_bytes=60 * 2**20,
        ),
        name="layer_rest",
    )(tokens, *small, *matrices)


def rotation(positions, width):
    freqs = THETA ** (-jnp.arange(0, width, 2, dtype=jnp.float32) / width)
    angles = freqs[:, None] * positions.astype(jnp.float32)[None, :]
    return (jnp.cos(angles), jnp.sin(angles))


def body(
    tokens,
    pre_gain,
    outer_gate_weight,
    inner_gate_weight,
    source_weight,
    conv_taps,
    q_down_weight,
    q_norm_gain,
    q_up_weight,
    kv_down_weight,
    rope_key_weight,
    kv_norm_gain,
    kv_up_weight,
    attn_out_weight,
    conv_out_weight,
    post_gain,
):
    token_rows = tokens.shape[0]
    query_pos = lax.axis_index("sp") * token_rows + jnp.arange(token_rows, dtype=jnp.int32)
    cosine, sine = rotation(query_pos, ROPE)
    small = (
        pre_gain[None, :], conv_taps, q_norm_gain.reshape(-1, 128), kv_norm_gain[None, :], post_gain[None, :],
        rope_key_weight.T, cosine, sine,
    )
    matrices = (
        outer_gate_weight, inner_gate_weight, source_weight, q_down_weight, kv_down_weight,
        q_up_weight, kv_up_weight, attn_out_weight, conv_out_weight,
    )
    return layer(tokens, small, matrices)


def solution(mesh):
    placed = (
        P("sp", "tp"),
        P(),
        P(None, "tp"),
        P(None, "tp"),
        P(None, "tp"),
        P(None, "tp"),
        P(),
        P(),
        P(None, "tp"),
        P(),
        P(),
        P(),
        P(None, "tp"),
        P("tp", None),
        P("tp", None),
        P("tp"),
    )
    return jax.shard_map(
        body, mesh=mesh, in_specs=placed, out_specs=(P("sp", "tp"), P("tp", "sp")), check_vma=False
    )
```
